256 devices in a mesh: dp: 4 (over y), kv: 32 (over z, x), tp: 2 (over core).
Axes of the slice: x: 4, y: 4, z: 8, core: 2. Of those that a mesh axis runs over, the one named last changes fastest.
Arguments:
- tokens: bfloat16 [16, 4096], P('dp', 'kv'), may hold values from -18 to 18
- norm_gain: float32 [4096], P('kv'), may hold values from 0.1 to 1.9
- query_weight: bfloat16 [4096, 4096], P('kv', 'tp'), may hold values from -0.09375 to 0.09375
- key_weight: bfloat16 [4096, 512], P('kv', 'tp'), may hold values from -0.09375 to 0.09375
- value_weight: bfloat16 [4096, 512], P('kv', 'tp'), may hold values from -0.09375 to 0.09375
- gate_weight: bfloat16 [4096, 8], replicated, may hold values from -0.09375 to 0.09375
- gate_bias: float32 [8], replicated, may hold values from -2.5 to 0.5
- query_gain: float32 [64], replicated, may hold values from 0.1 to 1.9
- key_gain: float32 [64], replicated, may hold values from 0.1 to 1.9
- key_cache: bfloat16 [16, 65536, 512], P('dp', 'kv', 'tp'), may hold values from -6 to 6
- value_cache: bfloat16 [16, 65536, 512], P('dp', 'kv', 'tp'), may hold values from -9 to 9
- gate_cache: float32 [16, 8, 65536], P('dp', 'tp', 'kv'), may hold values from -65536 to 0, as said below
- lengths: int32 [16], P('dp'), may hold values from 32769 to 65536, as said below
- out_weight: bfloat16 [4096, 4096], P('tp', 'kv'), may hold values from -0.75 to 0.75
Outputs:
- mixed: bfloat16 [16, 4096], P('dp', 'kv')
The draws below stay inside these ranges and needn't reach their ends.
Inputs may be any that keep to these rules, and one draw needn't show every extreme that they name: `gate_cache`: never rising along positions. `lengths`: in every draw some sequence has all 65536 positions cached.
All inputs are finite; a program needn't handle non-finite values.
Results may differ from the reference program's by a relative error of at most 0.012.
Values may be sent and summed in bfloat16 or wider, within the bound.
No kernel may reach another device: no remote copies, remote signals or barrier semaphores. Data moves between devices by JAX's collectives and lax.ppermute only.
A program may use at most 64 MiB of HBM per device.

```python
import math
import jax
import jax.numpy as jnp
from jax import lax

D = 4096
HEADS = 64
KV_HEADS = 8
HEAD = 64
POS_DEV = 2048
BATCH = 16
SPAN = 65536
N_KV = 32
N_TP = 2


def draw_tokens(key, part):
    first, second, third = jax.random.split(key, 3)
    width = max(D // 32, 1)
    base = jnp.clip(jax.random.normal(first, (BATCH, D), jnp.float32), -6.0, 6.0)
    scales = jnp.exp(jax.random.uniform(second, (BATCH, D // width), jnp.float32, -1.09, 1.09))
    return (base * jnp.repeat(scales, width, axis=1)).astype(jnp.bfloat16)


def draw_value_cache(key, part):
    first, second = jax.random.split(key, 2)
    channels = KV_HEADS * HEAD
    block = max(POS_DEV // 4, 1)
    blocks = SPAN // block
    offsets = jnp.clip(jax.random.normal(second, (BATCH, blocks, 1, channels), jnp.float32), -3.0, 3.0)
    base = jnp.clip(jax.random.normal(first, (BATCH, blocks, block, channels), jnp.float32), -6.0, 6.0)
    return (base + offsets).reshape(BATCH, SPAN, channels).astype(jnp.bfloat16)


def draw_gate_cache(key, part):
    keys = jax.random.split(key, 6)
    share = 0.5
    flags = jax.random.uniform(keys[0], (BATCH, KV_HEADS), jnp.float32) < share
    forced = jax.random.randint(keys[1], (), 0, BATCH * KV_HEADS)
    flags = flags | (jnp.arange(BATCH * KV_HEADS).reshape(BATCH, KV_HEADS) == forced)
    fast = jnp.exp(jax.random.uniform(keys[2], (BATCH, KV_HEADS), jnp.float32, math.log(0.01), math.log(0.033)))
    slow = jnp.exp(jax.random.uniform(keys[3], (BATCH, KV_HEADS), jnp.float32, math.log(0.3), math.log(1.5))) / SPAN
    rate = jnp.where(flags, fast, slow)
    block = max(POS_DEV // 2, 1)
    blocks = SPAN // block
    factor = jnp.exp(jax.random.uniform(keys[4], (BATCH, KV_HEADS, blocks, 1), jnp.float32, math.log(0.35), math.log(2.8)))
    rough = jax.random.uniform(keys[5], (BATCH, KV_HEADS, blocks, block), jnp.float32, 0.5, 1.5)
    steps = -(rate[:, :, None, None] * factor * rough).reshape(BATCH, KV_HEADS, SPAN)
    return jnp.cumsum(steps, axis=2)


def draw_lengths(key, part):
    first, second = jax.random.split(key, 2)
    lengths = SPAN - jax.random.randint(first, (BATCH,), 0, SPAN // 2)
    chosen = jax.random.randint(second, (), 0, BATCH)
    return jnp.where(jnp.arange(BATCH) == chosen, SPAN, lengths).astype(jnp.int32)


def level_of(rng, extent, cuts, low, top_value):
    level, own = 1.0, jax.random.fold_in(rng, 6)
    for dim, shards_of in cuts:
        draws = jnp.exp(jax.random.uniform(jax.random.fold_in(own, dim), (shards_of,), jnp.float32, low / len(cuts), top_value / len(cuts)))
        level = level * jnp.repeat(draws, extent[dim] // shards_of).reshape([-1 if axis == dim else 1 for axis in range(len(extent))])
    return level


def bell_draw(own_key, dims, spread, limit, cuts=(), kind=jnp.bfloat16):
    level = level_of(own_key, dims, cuts, -0.22, 0.18) if cuts else 1.0
    array = jax.random.normal(own_key, dims, jnp.float32) * spread * level
    return jnp.minimum(jnp.maximum(array, -limit), limit).astype(kind)


def setup_inputs(seed: int = 0) -> dict:
    key_of = jax.random.split(jax.random.key(seed), 15)
    return {
        "tokens": draw_tokens(jax.random.fold_in(key_of[14], 71), 0),
        "norm_gain": jnp.clip(1.0 + 0.18 * jax.random.normal(key_of[1], (D,), jnp.float32), 0.1, 1.9),
        "query_weight": bell_draw(key_of[2], (D, HEADS * HEAD), D ** -0.5, 0.09375, ((0, 32), (1, 2))),
        "key_weight": bell_draw(key_of[3], (D, KV_HEADS * HEAD), D ** -0.5, 0.09375, ((0, 32), (1, 2))),
        "value_weight": bell_draw(key_of[4], (D, KV_HEADS * HEAD), D ** -0.5, 0.09375, ((0, 32), (1, 2))),
        "gate_weight": bell_draw(key_of[5], (D, KV_HEADS), D ** -0.5, 0.09375),
        "gate_bias": jnp.clip(jax.random.uniform(key_of[6], (KV_HEADS,), jnp.float32, -2.5, 0.5), -2.5, 0.5),
        "query_gain": jnp.clip(1.0 + 0.18 * jax.random.normal(key_of[7], (HEAD,), jnp.float32), 0.1, 1.9),
        "key_gain": jnp.clip(1.0 + 0.18 * jax.random.normal(key_of[8], (HEAD,), jnp.float32), 0.1, 1.9),
        "key_cache": bell_draw(key_of[9], (BATCH, SPAN, KV_HEADS * HEAD), 1.0, 6.0, ((0, 4), (1, 32), (2, 2))),
        "value_cache": draw_value_cache(jax.random.fold_in(key_of[14], 71), 0),
        "gate_cache": draw_gate_cache(jax.random.fold_in(key_of[14], 71), 0),
        "lengths": draw_lengths(jax.random.fold_in(key_of[14], 71), 0),
        "out_weight": bell_draw(key_of[13], (HEADS * HEAD, D), HEAD ** -0.5, 0.75, ((0, 2), (1, 32))),
    }


EPSILON = 1e-06
FLOOR = -1e+30

def head_norm(values, gain):
    values = values.astype(jnp.float32)
    return values * lax.rsqrt(lax.optimization_barrier(jnp.mean(values * values, axis=-1, keepdims=True)) + EPSILON) * gain

def one_sequence(inputs):
    queries, key_new, value_new, log_gate, key_rows, value_rows, gate_rows, length = inputs
    scale = HEAD ** (-0.5)
    keys = key_rows.reshape(N_KV, POS_DEV, KV_HEADS, HEAD).astype(jnp.float32)
    values = value_rows.reshape(N_KV, POS_DEV, KV_HEADS, HEAD).astype(jnp.float32)
    gates = gate_rows.reshape(KV_HEADS, N_KV, POS_DEV).transpose(1, 0, 2)
    queries_f = queries.astype(jnp.float32)
    scores = jnp.einsum('grd,bpgd->bgrp', queries_f, keys) * scale - gates[:, :, None, :]
    places = jnp.arange(SPAN, dtype=jnp.int32).reshape(N_KV, POS_DEV)
    live = (places < length)[:, None, None, :]
    last = (length - 1).astype(jnp.int32)
    last_gate = lax.dynamic_slice_in_dim(gate_rows, last, 1, 1)[:, 0]
    own_gate = last_gate + log_gate
    score_new = jnp.einsum('grd,gd->gr', queries_f, key_new.astype(jnp.float32)) * scale - own_gate[:, None]
    owner = (jnp.arange(N_KV, dtype=jnp.int32) == last // POS_DEV)[:, None, None]
    block_max = lax.optimization_barrier(jnp.max(jnp.where(live, scores, FLOOR), axis=3))
    block_max = jnp.where(owner, jnp.maximum(block_max, score_new[None]), block_max)
    weights = jnp.where(live, jnp.exp(scores - block_max[..., None]), 0.0).astype(jnp.bfloat16)
    weights = lax.optimization_barrier(weights).astype(jnp.float32)
    weight_new = jnp.where(owner, jnp.exp(score_new[None] - block_max), 0.0).astype(jnp.bfloat16)
    weight_new = lax.optimization_barrier(weight_new).astype(jnp.float32)
    block_sum = lax.optimization_barrier(jnp.sum(weights, axis=3)) + weight_new
    block_values = jnp.einsum('bgrp,bpgd->bgrd', weights, values)
    block_values = block_values + weight_new[..., None] * value_new.astype(jnp.float32)[None, :, None, :]
    top = lax.optimization_barrier(jnp.max(block_max, axis=0))
    factor = jnp.exp(block_max - top)
    total = lax.optimization_barrier(jnp.sum(factor * block_sum, axis=0))
    summed = lax.optimization_barrier(jnp.sum(factor[..., None] * block_values, axis=0))
    return (summed / total[..., None]).astype(jnp.bfloat16).reshape(HEADS * HEAD)

def reference(tokens, norm_gain, query_weight, key_weight, value_weight, gate_weight, gate_bias, query_gain, key_gain, key_cache, value_cache, gate_cache, lengths, out_weight):
    count = tokens.shape[0]
    ratio = HEADS // KV_HEADS
    tokens_f = tokens.astype(jnp.float32)
    inverse = lax.rsqrt(lax.optimization_barrier(jnp.sum(tokens_f * tokens_f, axis=1)) / D + EPSILON)[:, None]
    scaled = (tokens_f * norm_gain).astype(jnp.bfloat16)
    query_raw = (jnp.dot(scaled, query_weight, preferred_element_type=jnp.float32) * inverse).astype(jnp.bfloat16)
    key_raw = (jnp.dot(scaled, key_weight, preferred_element_type=jnp.float32) * inverse).astype(jnp.bfloat16)
    value_new = (jnp.dot(scaled, value_weight, preferred_element_type=jnp.float32) * inverse).astype(jnp.bfloat16)
    log_gate = jax.nn.log_sigmoid(jnp.dot(scaled, gate_weight, preferred_element_type=jnp.float32) * inverse + gate_bias)
    queries = head_norm(query_raw.reshape(count, KV_HEADS, ratio, HEAD), query_gain).astype(jnp.bfloat16)
    key_new = head_norm(key_raw.reshape(count, KV_HEADS, HEAD), key_gain).astype(jnp.bfloat16)
    attended = lax.map(one_sequence, (queries, key_new, value_new.reshape(count, KV_HEADS, HEAD), log_gate, key_cache, value_cache, gate_cache, lengths))
    rows = HEADS * HEAD // N_TP
    total = jnp.zeros((count, D), jnp.float32)
    for group in range(N_TP):
        part = jnp.dot(attended[:, group * rows:(group + 1) * rows], out_weight[group * rows:(group + 1) * rows], preferred_element_type=jnp.float32).astype(jnp.bfloat16)
        total = total + lax.optimization_barrier(part).astype(jnp.float32)
    return total.astype(jnp.bfloat16)
```

```python
import functools

import jax
import jax.numpy as jnp
from jax import lax
from jax.experimental import pallas as pl
from jax.experimental.pallas import tpu as pltpu
from jax.sharding import Mesh
from jax.sharding import PartitionSpec as P

D = 4096
HEADS = 64
KV_HEADS = 8
HEAD = 64
KV = ("kv_0", "kv_1")

EPSILON = 1e-06
FLOOR = -1e30
VMEM = pltpu.VMEM
F32 = jnp.float32
BF16 = jnp.bfloat16


def lanes_of(shape):
    return lax.broadcasted_iota(jnp.int32, shape, 1)


def halves_stacked(part):
    half = part.shape[1] // 2
    return jnp.concatenate([part[:, :half], part[:, half:]], axis=0)


def project_kernel(tokens_ref, gain_ref, query_ref, key_ref, value_ref, gate_ref, out_ref):
    tokens = tokens_ref[...].astype(F32)
    squares = jnp.sum(tokens * tokens, axis=1, keepdims=True)
    scaled = (tokens * gain_ref[...]).astype(BF16)
    query = jnp.dot(scaled, query_ref[...], preferred_element_type=F32)
    key = jnp.dot(scaled, key_ref[...], preferred_element_type=F32)
    value = jnp.dot(scaled, value_ref[...], preferred_element_type=F32)
    gate = jnp.dot(scaled, gate_ref[...], preferred_element_type=F32)
    extra = gate + jnp.where(lanes_of(gate.shape) == 4, squares, 0.0)
    extra = jnp.concatenate([extra, jnp.zeros_like(extra)], axis=0)
    whole = jnp.concatenate(
        [halves_stacked(query), halves_stacked(key), halves_stacked(value), extra], axis=1
    ).astype(BF16)
    for copy in range(out_ref.shape[0]):
        out_ref[copy] = whole


def split_heads_sum(squares):
    row = lax.broadcasted_iota(jnp.int32, (128, 128), 0) // HEAD
    column = lanes_of((128, 128)) // HEAD
    ones = jnp.where(row == column, 1.0, 0.0).astype(BF16)
    high = squares.astype(BF16)
    low = (squares - high.astype(F32)).astype(BF16)
    return jnp.dot(high, ones, preferred_element_type=F32) + jnp.dot(
        low, ones, preferred_element_type=F32
    )


def attend_kernel(
    rest_ref, sums_ref, small_ref, gate_ref, key_ref, value_ref, out_ref, query_ref
):
    seqs, positions = gate_ref.shape[0], gate_ref.shape[2]
    total = sums_ref[0].astype(F32)
    for piece in range(1, sums_ref.shape[0]):
        total = total + sums_ref[piece].astype(F32)
    extra = total[:, 1280:]
    inverse = lax.rsqrt(extra[0:seqs, 4:5] / D + EPSILON)
    inverse = jnp.concatenate([inverse, inverse], axis=0)
    raw = (total[:, :1280] * inverse).astype(BF16).astype(F32)
    tiles = [raw[:, 128 * k : 128 * (k + 1)] for k in range(10)]
    values_new = tiles[9]
    stacked = jnp.concatenate(tiles[:9], axis=0)
    mean = split_heads_sum(stacked * stacked) * (1.0 / HEAD)
    normed = stacked * lax.rsqrt(mean + EPSILON)
    query_ref[...] = (normed[:64] * small_ref[0:1, :]).astype(BF16).astype(F32)
    keys_new = (normed[64:] * small_ref[1:2, :]).astype(BF16).astype(F32)
    logit = extra * inverse + small_ref[2:3, :]
    log_gate = jnp.minimum(logit, 0.0) - jnp.log1p(jnp.exp(-jnp.abs(logit)))

    lane = lanes_of((8, 128))
    row = lax.broadcasted_iota(jnp.int32, (8, 128), 0)
    left, early = lane < HEAD, row < 4
    place = lanes_of((8, positions))
    early_wide = lax.broadcasted_iota(jnp.int32, (8, positions), 0) < 4
    maxima = jnp.zeros((8, 128), F32)
    sums = jnp.zeros((8, 128), F32)
    for s in range(seqs):
        rest = rest_ref[s]
        owner = jnp.logical_and(rest >= 1, rest <= positions)
        live = place < rest
        chosen = place == rest - 1
        parts, gates, last, fresh = [], [], [], []
        for a in range(2):
            heads = query_ref[pl.ds(a * seqs + s, 8, stride=8), :]
            turned = pltpu.roll(heads, HEAD, 1)
            even = jnp.where(left == early, jnp.where(early, heads, turned), 0.0)
            odd = jnp.where(left == early, jnp.where(early, turned, heads), 0.0)
            parts.append(jnp.concatenate([even, odd], axis=0) * HEAD ** (-0.5))
            gate = jnp.where(
                early_wide, gate_ref[s, 2 * a : 2 * a + 1, :], gate_ref[s, 2 * a + 1 : 2 * a + 2, :]
            )
            gates.append(gate)
            own = jnp.sum(jnp.where(chosen, gate, 0.0), axis=1, keepdims=True)
            wanted = jnp.where(early, 2 * a, 2 * a + 1)
            own = own + jnp.sum(
                jnp.where(lane == wanted, log_gate[s : s + 1, :], 0.0), axis=1, keepdims=True
            )
            new = jnp.sum(
                parts[a] * keys_new[a * seqs + s : a * seqs + s + 1, :], axis=1, keepdims=True
            )
            fresh.append(new - jnp.concatenate([own, own], axis=0))
        zeros = jnp.zeros((16, 128), F32)
        query = jnp.concatenate(
            [
                jnp.concatenate([parts[0], zeros], axis=1),
                jnp.concatenate([zeros, parts[1]], axis=1),
            ],
            axis=0,
        ).astype(BF16)
        scores = lax.dot_general(
            query, key_ref[s], (((1,), (1,)), ((), ())), preferred_element_type=F32
        )
        gate = jnp.concatenate([gates[0], gates[0], gates[1], gates[1]], axis=0)
        live = jnp.concatenate([live] * 4, axis=0)
        scores = jnp.where(live, scores - gate, FLOOR)
        top = jnp.max(scores, axis=1, keepdims=True)
        score_new = jnp.concatenate(fresh, axis=0)
        top = jnp.where(owner, jnp.maximum(top, score_new), top)
        weights = jnp.where(live, jnp.exp(scores - top), 0.0).astype(BF16)
        weight_new = jnp.where(owner, jnp.exp(score_new - top), 0.0).astype(BF16).astype(F32)
        count = jnp.sum(weights.astype(F32), axis=1, keepdims=True) + weight_new
        summed = jnp.dot(weights, value_ref[s], preferred_element_type=F32)
        for a in range(2):
            rows = slice(16 * a, 16 * a + 16)
            mine = summed[rows, 128 * a : 128 * a + 128]
            mine = mine + weight_new[rows] * values_new[a * seqs + s : a * seqs + s + 1, :]
            even, odd = mine[:8], mine[8:]
            dense = jnp.where(
                left,
                jnp.where(early, even, pltpu.roll(even, HEAD, 1)),
                jnp.where(early, pltpu.roll(odd, HEAD, 1), odd),
            ).astype(BF16)
            at = 8 * (2 * s + a)
            for copy in range(out_ref.shape[0]):
                out_ref[copy, at : at + 8, :] = dense
            for p in range(2):
                here = lane == 4 * s + 2 * a + p
                own_rows = slice(16 * a + 8 * p, 16 * a + 8 * p + 8)
                maxima = jnp.where(here, top[own_rows], maxima)
                sums = jnp.where(here, count[own_rows], sums)
    packed = pack_statistics(maxima, sums)
    for copy in range(out_ref.shape[0]):
        out_ref[copy, 64:72, :] = packed


def pack_statistics(maxima, sums):
    first = maxima.astype(BF16).astype(F32)
    second = (maxima - first).astype(BF16).astype(F32)
    third = (maxima - first - second).astype(BF16).astype(F32)
    high = sums.astype(BF16).astype(F32)
    low = (sums - high).astype(BF16).astype(F32)
    packed = first + pltpu.roll(second, 16, 1) + pltpu.roll(third, 32, 1)
    packed = packed + pltpu.roll(high, 48, 1) + pltpu.roll(low, 64, 1)
    return packed.astype(BF16)


def unpack_statistics(packed):
    packed = packed.astype(F32)
    valid = lanes_of((8, 128)) < 16
    maxima = packed + pltpu.roll(packed, 112, 1) + pltpu.roll(packed, 96, 1)
    sums = pltpu.roll(packed, 80, 1) + pltpu.roll(packed, 64, 1)
    return jnp.where(valid, maxima, 0.0), jnp.where(valid, sums, 0.0)


def spread(tile, k):
    left = lanes_of((8, 128)) < HEAD
    return jnp.where(left, tile[:, 2 * k : 2 * k + 1], tile[:, 2 * k + 1 : 2 * k + 2])


def merged(in_ref):
    pieces = in_ref.shape[0]
    found = [unpack_statistics(in_ref[i, 64:72, :]) for i in range(pieces)]
    top = functools.reduce(jnp.maximum, [maxima for maxima, _ in found])
    factors = [jnp.exp(maxima - top) for maxima, _ in found]
    total = sum(factor * sums for factor, (_, sums) in zip(factors, found))
    values = []
    for k in range(8):
        values.append(
            sum(
                in_ref[i, 8 * k : 8 * k + 8, :].astype(F32) * spread(factors[i], k)
                for i in range(pieces)
            )
        )
    return top, total, values


def merge_kernel(in_ref, out_ref):
    top, total, values = merged(in_ref)
    packed = pack_statistics(top, total)
    dense = jnp.concatenate(values, axis=0).astype(BF16)
    for copy in range(out_ref.shape[0]):
        out_ref[copy, :64, :] = dense
        out_ref[copy, 64:72, :] = packed


def finish_kernel(in_ref, weight_ref, out_ref, attended_ref):
    top, total, values = merged(in_ref)
    for k in range(8):
        attended_ref[8 * k : 8 * k + 8, :] = values[k] / spread(total, k)
    attended = jnp.concatenate(
        [attended_ref[pl.ds(k, 4, stride=16), :] for k in range(16)], axis=1
    ).astype(BF16)
    out_ref[...] = jnp.dot(attended, weight_ref[...], preferred_element_type=F32).astype(BF16)


def limit(mebibytes):
    return pltpu.CompilerParams(vmem_limit_bytes=mebibytes << 20)


def in_vmem(count):
    return [pl.BlockSpec(memory_space=VMEM)] * count


def exchanged(array, axis):
    return lax.all_to_all(array, axis, 0, 0, tiled=True)


def per_device(
    tokens,
    norm_gain,
    query_weight,
    key_weight,
    value_weight,
    gate_weight,
    gate_bias,
    query_gain,
    key_gain,
    key_cache,
    value_cache,
    gate_cache,
    lengths,
    out_weight,
):
    seqs, columns = tokens.shape
    kv_rank = lax.axis_index(KV)
    tp_rank = lax.axis_index("tp")
    groups = key_weight.shape[1] // HEAD
    positions = key_cache.shape[1]
    outer, inner = lax.axis_size("kv_0"), lax.axis_size("kv_1")
    gate_rows = lax.dynamic_slice(
        gate_weight, (kv_rank * columns, tp_rank * groups), (columns, groups)
    )
    gate_rows = jnp.pad(gate_rows, ((0, 0), (0, 128 - groups)))
    local_bias = lax.dynamic_slice_in_dim(gate_bias, tp_rank * groups, groups)
    small = jnp.stack(
        [jnp.tile(query_gain, 2), jnp.tile(key_gain, 2), jnp.pad(local_bias, (0, 128 - groups))]
    )
    rest = lengths - kv_rank * positions

    sums = pl.pallas_call(
        project_kernel,
        out_shape=jax.ShapeDtypeStruct((inner, 8, 1408), BF16),
        in_specs=in_vmem(6),
        out_specs=in_vmem(1)[0],
        compiler_params=limit(4),
        name="project",
    )(tokens, norm_gain[None], query_weight, key_weight, value_weight, gate_rows)
    sums = exchanged(sums, "kv_1").astype(F32).sum(0).astype(BF16)
    sums = exchanged(jnp.broadcast_to(sums[None], (outer, 8, 1408)), "kv_0")
    parts = pl.pallas_call(
        attend_kernel,
        out_shape=jax.ShapeDtypeStruct((inner, 72, 128), BF16),
        in_specs=[pl.BlockSpec(memory_space=pltpu.SMEM)] + in_vmem(5),
        out_specs=in_vmem(1)[0],
        scratch_shapes=[VMEM((64, 128), F32)],
        compiler_params=limit(24),
        name="attend",
    )(rest, sums, small, gate_cache, key_cache, value_cache)
    parts = pl.pallas_call(
        merge_kernel,
        out_shape=jax.ShapeDtypeStruct((outer, 72, 128), BF16),
        in_specs=in_vmem(1),
        out_specs=in_vmem(1)[0],
        compiler_params=limit(4),
        name="merge",
    )(exchanged(parts, "kv_1"))
    mixed = pl.pallas_call(
        finish_kernel,
        out_shape=jax.ShapeDtypeStruct((seqs, out_weight.shape[1]), BF16),
        in_specs=in_vmem(2),
        out_specs=in_vmem(1)[0],
        scratch_shapes=[VMEM((64, 128), F32)],
        compiler_params=limit(4),
        name="finish",
    )(exchanged(parts, "kv_0"), out_weight)
    other = lax.ppermute(mixed, "tp", [(0, 1), (1, 0)])
    return (mixed.astype(F32) + other.astype(F32)).astype(BF16)


def solution(mesh):
    finer = Mesh(
        mesh.devices.reshape(mesh.shape["dp"], 8, 4, mesh.shape["tp"]), ("dp", "kv_0", "kv_1", "tp")
    )
    in_specs = (
        P("dp", KV),
        P(KV),
        P(KV, "tp"),
        P(KV, "tp"),
        P(KV, "tp"),
        P(),
        P(),
        P(),
        P(),
        P("dp", KV, "tp"),
        P("dp", KV, "tp"),
        P("dp", "tp", KV),
        P("dp"),
        P("tp", KV),
    )
    out_specs = P("dp", KV)
    return jax.shard_map(
        per_device, mesh=finer, in_specs=in_specs, out_specs=out_specs, check_vma=False
    )
```

```python
import functools

import jax
import jax.numpy as jnp
from jax import lax
from jax.experimental import pallas as pl
from jax.experimental.pallas import tpu as pltpu
from jax.sharding import Mesh
from jax.sharding import PartitionSpec as P

D = 4096
HEADS = 64
KV_HEADS = 8
HEAD = 64
POSITIONS = 2048
KV = ("kv_0", "kv_1")

EPSILON = 1e-06
FLOOR = -1e30
VMEM = pltpu.VMEM
F32 = jnp.float32
BF16 = jnp.bfloat16


def lanes_of(shape):
    return lax.broadcasted_iota(jnp.int32, shape, 1)


def halves_stacked(part):
    half = part.shape[1] // 2
    return jnp.concatenate([part[:, :half], part[:, half:]], axis=0)


def project_kernel(
    tokens_hbm,
    norm_gain_hbm,
    query_hbm,
    key_hbm,
    value_hbm,
    gate_hbm,
    bias_hbm,
    query_gain_hbm,
    key_gain_hbm,
    lengths_hbm,
    out_ref,
    small_ref,
    tokens_ref,
    norm_gain_ref,
    query_ref,
    key_ref,
    value_ref,
    gate_ref,
    bias_ref,
    query_gain_ref,
    key_gain_ref,
    lengths_ref,
    arrived,
):
    kv_rank = lax.axis_index(KV)
    columns = tokens_ref.shape[1]
    mine = pl.ds(pl.multiple_of(kv_rank * columns, columns), columns)
    pairs = [
        (tokens_hbm, tokens_ref),
        (norm_gain_hbm, norm_gain_ref),
        (query_hbm, query_ref),
        (key_hbm, key_ref),
        (value_hbm, value_ref),
        (gate_hbm.at[:, mine], gate_ref),
        (bias_hbm, bias_ref),
        (query_gain_hbm, query_gain_ref),
        (key_gain_hbm, key_gain_ref),
        (lengths_hbm, lengths_ref),
    ]
    copies = [pltpu.make_async_copy(*pair, arrived.at[k]) for k, pair in enumerate(pairs)]
    for copy in copies:
        copy.start()
    for copy in copies:
        copy.wait()
    tokens = tokens_ref[...].astype(F32)
    squares = jnp.sum(tokens * tokens, axis=1, keepdims=True)
    scaled = (tokens * norm_gain_ref[...]).astype(BF16)
    query = jnp.dot(scaled, query_ref[...], preferred_element_type=F32)
    key = jnp.dot(scaled, key_ref[...], preferred_element_type=F32)
    value = jnp.dot(scaled, value_ref[...], preferred_element_type=F32)
    rows = jnp.concatenate([gate_ref[...].astype(F32), jnp.zeros((120, 128), F32)], axis=0)
    gate = lax.dot_general(
        scaled, rows.astype(BF16), (((1,), (1,)), ((), ())), preferred_element_type=F32
    )
    extra = gate + jnp.where(lanes_of(gate.shape) == KV_HEADS, squares, 0.0)
    extra = jnp.concatenate([extra, jnp.zeros_like(extra)], axis=0)
    whole = jnp.concatenate(
        [halves_stacked(query), halves_stacked(key), halves_stacked(value), extra], axis=1
    ).astype(BF16)
    for copy in range(out_ref.shape[0]):
        out_ref[copy] = whole
    small_ref[0:1, :] = jnp.concatenate([query_gain_ref[...]] * 2, axis=1)
    small_ref[1:2, :] = jnp.concatenate([key_gain_ref[...]] * 2, axis=1)
    small_ref[2:3, :] = jnp.zeros((1, 128), F32)
    small_ref[2:3, 0 : bias_ref.shape[1]] = bias_ref[...]
    rest = lengths_ref[...] - kv_rank * POSITIONS
    small_ref[3:4, :] = jnp.zeros((1, 128), F32)
    small_ref[3:4, 0 : rest.shape[1]] = rest.astype(F32)


def split_heads_sum(squares):
    row = lax.broadcasted_iota(jnp.int32, (128, 128), 0) // HEAD
    column = lanes_of((128, 128)) // HEAD
    ones = jnp.where(row == column, 1.0, 0.0).astype(BF16)
    high = squares.astype(BF16)
    low = (squares - high.astype(F32)).astype(BF16)
    return jnp.dot(high, ones, preferred_element_type=F32) + jnp.dot(
        low, ones, preferred_element_type=F32
    )


def fold_kernel(in_ref, out_ref):
    total = in_ref[0].astype(F32)
    for piece in range(1, in_ref.shape[0]):
        total = total + in_ref[piece].astype(F32)
    total = total.astype(BF16)
    for copy in range(out_ref.shape[0]):
        out_ref[copy] = total


def attend_kernel(
    sums_ref,
    small_ref,
    gate_ref,
    key_ref,
    value_ref,
    out_ref,
    query_ref,
    scores_ref,
    weights_ref,
):
    tp_rank = lax.axis_index("tp")
    seqs, positions = gate_ref.shape[0], gate_ref.shape[2]
    total = sums_ref[0].astype(F32)
    for piece in range(1, sums_ref.shape[0]):
        total = total + sums_ref[piece].astype(F32)
    extra = total[:, 1280:]
    inverse = lax.rsqrt(extra[0:seqs, KV_HEADS : KV_HEADS + 1] / D + EPSILON)
    inverse = jnp.concatenate([inverse, inverse], axis=0)
    raw = (total[:, :1280] * inverse).astype(BF16).astype(F32)
    tiles = [raw[:, 128 * k : 128 * (k + 1)] for k in range(10)]
    values_new = tiles[9]
    stacked = jnp.concatenate(tiles[:9], axis=0)
    mean = split_heads_sum(stacked * stacked) * (1.0 / HEAD)
    normed = stacked * lax.rsqrt(mean + EPSILON)
    query_ref[...] = (normed[:64] * small_ref[0:1, :]).astype(BF16).astype(F32)
    keys_new = (normed[64:] * small_ref[1:2, :]).astype(BF16).astype(F32)
    logit = extra * inverse + small_ref[2:3, :]
    log_gate = jnp.minimum(logit, 0.0) - jnp.log1p(jnp.exp(-jnp.abs(logit)))

    lane = lanes_of((8, 128))
    left = lane < HEAD
    early = lax.broadcasted_iota(jnp.int32, (8, 128), 0) < 4
    blocks = positions // 128
    rest = [
        jnp.broadcast_to(small_ref[3:4, s : s + 1], (8, 128)).astype(jnp.int32)
        for s in range(seqs)
    ]
    owner = [jnp.logical_and(r >= 1, r <= positions) for r in rest]

    def gate_rows(s, a, j):
        part = slice(128 * j, 128 * j + 128)
        return jnp.where(
            early, gate_ref[s, 2 * a : 2 * a + 1, part], gate_ref[s, 2 * a + 1 : 2 * a + 2, part]
        )

    parts = {}
    for s in range(seqs):
        for a in range(2):
            heads = query_ref[pl.ds(a * seqs + s, 8, stride=8), :]
            turned = pltpu.roll(heads, HEAD, 1)
            even = jnp.where(left == early, jnp.where(early, heads, turned), 0.0)
            odd = jnp.where(left == early, jnp.where(early, turned, heads), 0.0)
            parts[s, a, 0] = even * HEAD ** (-0.5)
            parts[s, a, 1] = odd * HEAD ** (-0.5)
    zeros = jnp.zeros((16, 128), F32)
    for s in range(seqs):
        query = jnp.concatenate(
            [
                jnp.concatenate([parts[s, 0, 0], parts[s, 0, 1], zeros], axis=0),
                jnp.concatenate([zeros, parts[s, 1, 0], parts[s, 1, 1]], axis=0),
            ],
            axis=1,
        ).astype(BF16)
        scores_ref[32 * s : 32 * s + 32, :] = lax.dot_general(
            query, key_ref[s], (((1,), (1,)), ((), ())), preferred_element_type=F32
        )

    tops, owns = {}, {}
    for s in range(seqs):
        for a in range(2):
            tops[s, a, 0] = tops[s, a, 1] = jnp.full((8, 128), FLOOR, F32)
            owns[s, a] = jnp.zeros((8, 128), F32)
        for j in range(blocks):
            place = lane + 128 * j
            live, last = place < rest[s], place == rest[s] - 1
            for a in range(2):
                gate = gate_rows(s, a, j)
                owns[s, a] = owns[s, a] + jnp.where(last, gate, 0.0)
                for p in range(2):
                    at = 32 * s + 16 * a + 8 * p
                    score = scores_ref[at : at + 8, 128 * j : 128 * j + 128] - gate
                    score = jnp.where(live, score, FLOOR)
                    scores_ref[at : at + 8, 128 * j : 128 * j + 128] = score
                    tops[s, a, p] = jnp.maximum(tops[s, a, p], score)
    rows = [(s, a, p) for s in range(seqs) for a in range(2) for p in range(2)]
    fresh, top, weight_new = {}, {}, {}
    for s in range(seqs):
        for a in range(2):
            wanted = jnp.where(early, 2 * a, 2 * a + 1) + tp_rank * (KV_HEADS // 2)
            own = owns[s, a] + jnp.where(lane == wanted, log_gate[s : s + 1, :], 0.0)
            key_new = keys_new[a * seqs + s : a * seqs + s + 1, :]
            for p in range(2):
                fresh[s, a, p] = jnp.sum(parts[s, a, p] * key_new - own, axis=1, keepdims=True)
    for s, a, p in rows:
        most = jnp.max(tops[s, a, p], axis=1, keepdims=True)
        new = jnp.broadcast_to(fresh[s, a, p], (8, 128))
        most = jnp.broadcast_to(most, (8, 128))
        top[s, a, p] = jnp.where(owner[s], jnp.maximum(most, new), most)
        weight = jnp.where(owner[s], jnp.exp(new - top[s, a, p]), 0.0)
        weight_new[s, a, p] = weight.astype(BF16).astype(F32)
    counts = {}
    for s in range(seqs):
        for a in range(2):
            counts[s, a, 0] = counts[s, a, 1] = jnp.zeros((8, 128), F32)
        for j in range(blocks):
            live = lane + 128 * j < rest[s]
            for a in range(2):
                both = []
                for p in range(2):
                    at = 32 * s + 16 * a + 8 * p
                    score = scores_ref[at : at + 8, 128 * j : 128 * j + 128]
                    weight = jnp.where(live, jnp.exp(score - top[s, a, p]), 0.0).astype(BF16)
                    counts[s, a, p] = counts[s, a, p] + weight.astype(F32)
                    both.append(weight)
                at = 32 * s + 16 * a
                weights_ref[at : at + 16, 128 * j : 128 * j + 128] = jnp.concatenate(both, axis=0)
    summed = [
        jnp.dot(
            weights_ref[32 * s : 32 * s + 32, :], value_ref[s], preferred_element_type=F32
        )
        for s in range(seqs)
    ]
    maxima = jnp.zeros((8, 128), F32)
    sums = jnp.zeros((8, 128), F32)
    for s, a, p in rows:
        here = lane == 4 * s + 2 * a + p
        count = jnp.sum(counts[s, a, p], axis=1, keepdims=True) + weight_new[s, a, p]
        maxima = jnp.where(here, top[s, a, p], maxima)
        sums = jnp.where(here, count, sums)
    packed = pack_statistics(maxima, sums)
    for s in range(seqs):
        for a in range(2):
            new = values_new[a * seqs + s : a * seqs + s + 1, :]
            even, odd = (
                summed[s][16 * a + 8 * p : 16 * a + 8 * p + 8, 128 * a : 128 * a + 128]
                + weight_new[s, a, p] * new
                for p in range(2)
            )
            dense = jnp.where(
                left,
                jnp.where(early, even, pltpu.roll(even, HEAD, 1)),
                jnp.where(early, pltpu.roll(odd, HEAD, 1), odd),
            ).astype(BF16)
            at = 8 * (2 * s + a)
            for copy in range(out_ref.shape[0]):
                out_ref[copy, at : at + 8, :] = dense
    for copy in range(out_ref.shape[0]):
        out_ref[copy, 64:72, :] = packed


def pack_statistics(maxima, sums):
    first = maxima.astype(BF16).astype(F32)
    second = (maxima - first).astype(BF16).astype(F32)
    third = (maxima - first - second).astype(BF16).astype(F32)
    high = sums.astype(BF16).astype(F32)
    low = (sums - high).astype(BF16).astype(F32)
    packed = first + pltpu.roll(second, 16, 1) + pltpu.roll(third, 32, 1)
    packed = packed + pltpu.roll(high, 48, 1) + pltpu.roll(low, 64, 1)
    return packed.astype(BF16)


def unpack_statistics(packed):
    packed = packed.astype(F32)
    valid = lanes_of((8, 128)) < 16
    maxima = packed + pltpu.roll(packed, 112, 1) + pltpu.roll(packed, 96, 1)
    sums = pltpu.roll(packed, 80, 1) + pltpu.roll(packed, 64, 1)
    return jnp.where(valid, maxima, 0.0), jnp.where(valid, sums, 0.0)


def spread(tile, k):
    left = lanes_of((8, 128)) < HEAD
    return jnp.where(left, tile[:, 2 * k : 2 * k + 1], tile[:, 2 * k + 1 : 2 * k + 2])


def merged(in_ref):
    pieces = in_ref.shape[0]
    found = [unpack_statistics(in_ref[i, 64:72, :]) for i in range(pieces)]
    top = functools.reduce(jnp.maximum, [maxima for maxima, _ in found])
    factors = [jnp.exp(maxima - top) for maxima, _ in found]
    total = sum(factor * sums for factor, (_, sums) in zip(factors, found))
    values = []
    for k in range(8):
        values.append(
            sum(
                in_ref[i, 8 * k : 8 * k + 8, :].astype(F32) * spread(factors[i], k)
                for i in range(pieces)
            )
        )
    return top, total, values


def merge_kernel(in_ref, out_ref):
    top, total, values = merged(in_ref)
    packed = pack_statistics(top, total)
    dense = jnp.concatenate(values, axis=0).astype(BF16)
    for copy in range(out_ref.shape[0]):
        out_ref[copy, :64, :] = dense
        out_ref[copy, 64:72, :] = packed


def finish_kernel(in_ref, weight_ref, out_ref, attended_ref):
    top, total, values = merged(in_ref)
    for k in range(8):
        attended_ref[8 * k : 8 * k + 8, :] = values[k] / spread(total, k)
    attended = jnp.concatenate(
        [attended_ref[pl.ds(k, 4, stride=16), :] for k in range(16)], axis=1
    ).astype(BF16)
    out_ref[...] = jnp.dot(attended, weight_ref[...], preferred_element_type=F32).astype(BF16)


def limit(mebibytes):
    return pltpu.CompilerParams(vmem_limit_bytes=mebibytes << 20)


def in_vmem(count):
    return [pl.BlockSpec(memory_space=VMEM)] * count


def in_hbm(count):
    return [pl.BlockSpec(memory_space=pltpu.HBM)] * count


def held(*arrays):
    return [pltpu.with_memory_space_constraint(array, pltpu.HBM) for array in arrays]


def exchanged(array, axis):
    return lax.all_to_all(array, axis, 0, 0, tiled=True)


def per_device(
    tokens,
    norm_gain,
    query_weight,
    key_weight,
    value_weight,
    gate_weight,
    gate_bias,
    query_gain,
    key_gain,
    key_cache,
    value_cache,
    gate_cache,
    lengths,
    out_weight,
):
    seqs, columns = tokens.shape
    outer, inner = lax.axis_size("kv_0"), lax.axis_size("kv_1")
    sums, small = pl.pallas_call(
        project_kernel,
        out_shape=(
            jax.ShapeDtypeStruct((inner, 8, 1408), BF16),
            jax.ShapeDtypeStruct((8, 128), F32),
        ),
        in_specs=in_hbm(10),
        out_specs=tuple(in_vmem(2)),
        scratch_shapes=[
            VMEM(tokens.shape, BF16),
            VMEM((1, columns), F32),
            VMEM(query_weight.shape, BF16),
            VMEM(key_weight.shape, BF16),
            VMEM(value_weight.shape, BF16),
            VMEM((KV_HEADS, columns), BF16),
            VMEM((1, KV_HEADS), F32),
            VMEM((1, HEAD), F32),
            VMEM((1, HEAD), F32),
            VMEM((1, seqs), jnp.int32),
            pltpu.SemaphoreType.DMA((10,)),
        ],
        compiler_params=limit(4),
        name="project",
    )(
        *held(
            tokens,
            norm_gain[None],
            query_weight,
            key_weight,
            value_weight,
            gate_weight.T,
            gate_bias[None],
            query_gain[None],
            key_gain[None],
            lengths[None],
        )
    )
    sums = pl.pallas_call(
        fold_kernel,
        out_shape=jax.ShapeDtypeStruct((outer, 8, 1408), BF16),
        in_specs=in_vmem(1),
        out_specs=in_vmem(1)[0],
        compiler_params=limit(4),
        cost_estimate=pl.CostEstimate(
            flops=10**10, bytes_accessed=10**8, transcendentals=0
        ),
        name="fold",
    )(exchanged(sums, "kv_1"))
    parts = pl.pallas_call(
        attend_kernel,
        out_shape=jax.ShapeDtypeStruct((inner, 72, 128), BF16),
        in_specs=in_vmem(5),
        out_specs=in_vmem(1)[0],
        scratch_shapes=[
            VMEM((64, 128), F32),
            VMEM((32 * seqs, POSITIONS), F32),
            VMEM((32 * seqs, POSITIONS), BF16),
        ],
        compiler_params=limit(24),
        name="attend",
    )(exchanged(sums, "kv_0"), small, gate_cache, key_cache, value_cache)
    parts = pl.pallas_call(
        merge_kernel,
        out_shape=jax.ShapeDtypeStruct((outer, 72, 128), BF16),
        in_specs=in_vmem(1),
        out_specs=in_vmem(1)[0],
        compiler_params=limit(4),
        name="merge",
    )(exchanged(parts, "kv_1"))
    mixed = pl.pallas_call(
        finish_kernel,
        out_shape=jax.ShapeDtypeStruct((seqs, out_weight.shape[1]), BF16),
        in_specs=in_vmem(2),
        out_specs=in_vmem(1)[0],
        scratch_shapes=[VMEM((64, 128), F32)],
        compiler_params=limit(4),
        name="finish",
    )(exchanged(parts, "kv_0"), out_weight)
    other = lax.ppermute(mixed, "tp", [(0, 1), (1, 0)])
    return (mixed.astype(F32) + other.astype(F32)).astype(BF16)


def solution(mesh):
    finer = Mesh(
        mesh.devices.reshape(mesh.shape["dp"], 8, 4, mesh.shape["tp"]), ("dp", "kv_0", "kv_1", "tp")
    )
    in_specs = (
        P("dp", KV),
        P(KV),
        P(KV, "tp"),
        P(KV, "tp"),
        P(KV, "tp"),
        P(),
        P(),
        P(),
        P(),
        P("dp", KV, "tp"),
        P("dp", KV, "tp"),
        P("dp", "tp", KV),
        P("dp"),
        P("tp", KV),
    )
    out_specs = P("dp", KV)
    return jax.shard_map(
        per_device, mesh=finer, in_specs=in_specs, out_specs=out_specs, check_vma=False
    )
```

```python
import functools

import jax
import jax.numpy as jnp
from jax import lax
from jax.experimental import pallas as pl
from jax.experimental.pallas import tpu as pltpu
from jax.sharding import Mesh
from jax.sharding import PartitionSpec as P

D = 4096
HEADS = 64
KV_HEADS = 8
HEAD = 64
POSITIONS = 2048
KV = ("kv_0", "kv_1")


EPSILON = 1e-06
FLOOR = -1e30
VMEM = pltpu.VMEM
F32 = jnp.float32
BF16 = jnp.bfloat16


def lanes_of(shape):
    return lax.broadcasted_iota(jnp.int32, shape, 1)


def halves_stacked(part):
    half = part.shape[1] // 2
    return jnp.concatenate([part[:, :half], part[:, half:]], axis=0)


def project_kernel(
    tokens_hbm,
    norm_gain_hbm,
    query_hbm,
    key_hbm,
    value_hbm,
    gate_hbm,
    bias_hbm,
    query_gain_hbm,
    key_gain_hbm,
    lengths_hbm,
    out_ref,
    small_ref,
    tokens_ref,
    norm_gain_ref,
    query_ref,
    key_ref,
    value_ref,
    gate_ref,
    bias_ref,
    query_gain_ref,
    key_gain_ref,
    lengths_ref,
    arrived,
):
    kv_rank = lax.axis_index(KV)
    columns = tokens_ref.shape[1]
    mine = pl.ds(pl.multiple_of(kv_rank * columns, columns), columns)
    pairs = [
        (tokens_hbm, tokens_ref),
        (norm_gain_hbm, norm_gain_ref),
        (query_hbm, query_ref),
        (key_hbm, key_ref),
        (value_hbm, value_ref),
        (gate_hbm.at[:, mine], gate_ref),
        (bias_hbm, bias_ref),
        (query_gain_hbm, query_gain_ref),
        (key_gain_hbm, key_gain_ref),
        (lengths_hbm, lengths_ref),
    ]
    copies = [pltpu.make_async_copy(*pair, arrived.at[k]) for k, pair in enumerate(pairs)]
    for copy in copies:
        copy.start()
    for copy in copies:
        copy.wait()
    tokens = tokens_ref[...].astype(F32)
    squares = jnp.sum(tokens * tokens, axis=1, keepdims=True)
    scaled = (tokens * norm_gain_ref[...]).astype(BF16)
    query = jnp.dot(scaled, query_ref[...], preferred_element_type=F32)
    key = jnp.dot(scaled, key_ref[...], preferred_element_type=F32)
    value = jnp.dot(scaled, value_ref[...], preferred_element_type=F32)
    rows = jnp.concatenate([gate_ref[...].astype(F32), jnp.zeros((120, 128), F32)], axis=0)
    gate = lax.dot_general(
        scaled, rows.astype(BF16), (((1,), (1,)), ((), ())), preferred_element_type=F32
    )
    extra = gate + jnp.where(lanes_of(gate.shape) == KV_HEADS, squares, 0.0)
    extra = jnp.concatenate([extra, jnp.zeros_like(extra)], axis=0)
    whole = jnp.concatenate(
        [halves_stacked(query), halves_stacked(key), halves_stacked(value), extra], axis=1
    ).astype(BF16)
    out_ref[...] = whole
    small_ref[0:1, :] = jnp.concatenate([query_gain_ref[...]] * 2, axis=1)
    small_ref[1:2, :] = jnp.concatenate([key_gain_ref[...]] * 2, axis=1)
    small_ref[2:3, :] = jnp.zeros((1, 128), F32)
    small_ref[2:3, 0 : bias_ref.shape[1]] = bias_ref[...]
    rest = lengths_ref[...] - kv_rank * POSITIONS
    small_ref[3:4, :] = jnp.zeros((1, 128), F32)
    small_ref[3:4, 0 : rest.shape[1]] = rest.astype(F32)


def split_heads_sum(squares):
    row = lax.broadcasted_iota(jnp.int32, (128, 128), 0) // HEAD
    column = lanes_of((128, 128)) // HEAD
    ones = jnp.where(row == column, 1.0, 0.0).astype(BF16)
    high = squares.astype(BF16)
    low = (squares - high.astype(F32)).astype(BF16)
    return jnp.dot(high, ones, preferred_element_type=F32) + jnp.dot(
        low, ones, preferred_element_type=F32
    )


def fold_kernel(*refs):
    out_ref = refs[-1]
    total = sum(ref[...].astype(F32) for ref in refs[:-1]).astype(BF16)
    for copy in range(out_ref.shape[0]):
        out_ref[copy] = total


def attend_kernel(
    sums_ref,
    small_ref,
    gate_ref,
    key_ref,
    value_ref,
    out_ref,
    query_ref,
    scores_ref,
    weights_ref,
):
    tp_rank = lax.axis_index("tp")
    seqs, positions = gate_ref.shape[0], gate_ref.shape[2]
    total = sums_ref[0].astype(F32)
    for piece in range(1, sums_ref.shape[0]):
        total = total + sums_ref[piece].astype(F32)
    extra = total[:, 1280:]
    inverse = lax.rsqrt(extra[0:seqs, KV_HEADS : KV_HEADS + 1] / D + EPSILON)
    inverse = jnp.concatenate([inverse, inverse], axis=0)
    raw = (total[:, :1280] * inverse).astype(BF16).astype(F32)
    tiles = [raw[:, 128 * k : 128 * (k + 1)] for k in range(10)]
    values_new = tiles[9]
    stacked = jnp.concatenate(tiles[:9], axis=0)
    mean = split_heads_sum(stacked * stacked) * (1.0 / HEAD)
    normed = stacked * lax.rsqrt(mean + EPSILON)
    query_ref[...] = (normed[:64] * small_ref[0:1, :]).astype(BF16).astype(F32)
    keys_new = (normed[64:] * small_ref[1:2, :]).astype(BF16).astype(F32)
    logit = extra * inverse + small_ref[2:3, :]
    log_gate = jnp.minimum(logit, 0.0) - jnp.log1p(jnp.exp(-jnp.abs(logit)))

    lane = lanes_of((8, 128))
    left = lane < HEAD
    early = lax.broadcasted_iota(jnp.int32, (8, 128), 0) < 4
    blocks = positions // 128
    rest = [
        jnp.broadcast_to(small_ref[3:4, s : s + 1], (8, 128)).astype(jnp.int32)
        for s in range(seqs)
    ]
    owner = [jnp.logical_and(r >= 1, r <= positions) for r in rest]

    def gate_rows(s, a, j):
        part = slice(128 * j, 128 * j + 128)
        return jnp.where(
            early, gate_ref[s, 2 * a : 2 * a + 1, part], gate_ref[s, 2 * a + 1 : 2 * a + 2, part]
        )

    parts = {}
    for s in range(seqs):
        for a in range(2):
            heads = query_ref[pl.ds(a * seqs + s, 8, stride=8), :]
            turned = pltpu.roll(heads, HEAD, 1)
            even = jnp.where(left == early, jnp.where(early, heads, turned), 0.0)
            odd = jnp.where(left == early, jnp.where(early, turned, heads), 0.0)
            parts[s, a, 0] = even * HEAD ** (-0.5)
            parts[s, a, 1] = odd * HEAD ** (-0.5)
    zeros = jnp.zeros((16, 128), F32)
    for s in range(seqs):
        query = jnp.concatenate(
            [
                jnp.concatenate([parts[s, 0, 0], parts[s, 0, 1], zeros], axis=0),
                jnp.concatenate([zeros, parts[s, 1, 0], parts[s, 1, 1]], axis=0),
            ],
            axis=1,
        ).astype(BF16)
        scores_ref[32 * s : 32 * s + 32, :] = lax.dot_general(
            query, key_ref[s], (((1,), (1,)), ((), ())), preferred_element_type=F32
        )

    tops, owns = {}, {}
    for s in range(seqs):
        for a in range(2):
            tops[s, a, 0] = tops[s, a, 1] = jnp.full((8, 128), FLOOR, F32)
            owns[s, a] = jnp.zeros((8, 128), F32)
        for j in range(blocks):
            place = lane + 128 * j
            live, last = place < rest[s], place == rest[s] - 1
            for a in range(2):
                gate = gate_rows(s, a, j)
                owns[s, a] = owns[s, a] + jnp.where(last, gate, 0.0)
                for p in range(2):
                    at = 32 * s + 16 * a + 8 * p
                    score = scores_ref[at : at + 8, 128 * j : 128 * j + 128] - gate
                    score = jnp.where(live, score, FLOOR)
                    scores_ref[at : at + 8, 128 * j : 128 * j + 128] = score
                    tops[s, a, p] = jnp.maximum(tops[s, a, p], score)
    rows = [(s, a, p) for s in range(seqs) for a in range(2) for p in range(2)]
    fresh, top, weight_new = {}, {}, {}
    for s in range(seqs):
        for a in range(2):
            wanted = jnp.where(early, 2 * a, 2 * a + 1) + tp_rank * (KV_HEADS // 2)
            own = owns[s, a] + jnp.where(lane == wanted, log_gate[s : s + 1, :], 0.0)
            key_new = keys_new[a * seqs + s : a * seqs + s + 1, :]
            for p in range(2):
                fresh[s, a, p] = jnp.sum(parts[s, a, p] * key_new - own, axis=1, keepdims=True)
    for s, a, p in rows:
        most = jnp.max(tops[s, a, p], axis=1, keepdims=True)
        new = jnp.broadcast_to(fresh[s, a, p], (8, 128))
        most = jnp.broadcast_to(most, (8, 128))
        top[s, a, p] = jnp.where(owner[s], jnp.maximum(most, new), most)
        weight = jnp.where(owner[s], jnp.exp(new - top[s, a, p]), 0.0)
        weight_new[s, a, p] = weight.astype(BF16).astype(F32)
    counts = {}
    for s in range(seqs):
        for a in range(2):
            counts[s, a, 0] = counts[s, a, 1] = jnp.zeros((8, 128), F32)
        for j in range(blocks):
            live = lane + 128 * j < rest[s]
            for a in range(2):
                both = []
                for p in range(2):
                    at = 32 * s + 16 * a + 8 * p
                    score = scores_ref[at : at + 8, 128 * j : 128 * j + 128]
                    weight = jnp.where(live, jnp.exp(score - top[s, a, p]), 0.0).astype(BF16)
                    counts[s, a, p] = counts[s, a, p] + weight.astype(F32)
                    both.append(weight)
                at = 32 * s + 16 * a
                weights_ref[at : at + 16, 128 * j : 128 * j + 128] = jnp.concatenate(both, axis=0)
    summed = [
        jnp.dot(
            weights_ref[32 * s : 32 * s + 32, :], value_ref[s], preferred_element_type=F32
        )
        for s in range(seqs)
    ]
    maxima = jnp.zeros((8, 128), F32)
    sums = jnp.zeros((8, 128), F32)
    for s, a, p in rows:
        here = lane == 4 * s + 2 * a + p
        count = jnp.sum(counts[s, a, p], axis=1, keepdims=True) + weight_new[s, a, p]
        maxima = jnp.where(here, top[s, a, p], maxima)
        sums = jnp.where(here, count, sums)
    packed = pack_statistics(maxima, sums)
    for s in range(seqs):
        for a in range(2):
            new = values_new[a * seqs + s : a * seqs + s + 1, :]
            even, odd = (
                summed[s][16 * a + 8 * p : 16 * a + 8 * p + 8, 128 * a : 128 * a + 128]
                + weight_new[s, a, p] * new
                for p in range(2)
            )
            dense = jnp.where(
                left,
                jnp.where(early, even, pltpu.roll(even, HEAD, 1)),
                jnp.where(early, pltpu.roll(odd, HEAD, 1), odd),
            ).astype(BF16)
            at = 8 * (2 * s + a)
            out_ref[at : at + 8, :] = dense
    out_ref[64:72, :] = packed


def pack_statistics(maxima, sums):
    first = maxima.astype(BF16).astype(F32)
    second = (maxima - first).astype(BF16).astype(F32)
    third = (maxima - first - second).astype(BF16).astype(F32)
    high = sums.astype(BF16).astype(F32)
    low = (sums - high).astype(BF16).astype(F32)
    packed = first + pltpu.roll(second, 16, 1) + pltpu.roll(third, 32, 1)
    packed = packed + pltpu.roll(high, 48, 1) + pltpu.roll(low, 64, 1)
    return packed.astype(BF16)


def unpack_statistics(packed):
    packed = packed.astype(F32)
    valid = lanes_of((8, 128)) < 16
    maxima = packed + pltpu.roll(packed, 112, 1) + pltpu.roll(packed, 96, 1)
    sums = pltpu.roll(packed, 80, 1) + pltpu.roll(packed, 64, 1)
    return jnp.where(valid, maxima, 0.0), jnp.where(valid, sums, 0.0)


def spread(tile, k):
    left = lanes_of((8, 128)) < HEAD
    return jnp.where(left, tile[:, 2 * k : 2 * k + 1], tile[:, 2 * k + 1 : 2 * k + 2])


def merged(pieces):
    found = [unpack_statistics(piece[64:72, :]) for piece in pieces]
    top = functools.reduce(jnp.maximum, [maxima for maxima, _ in found])
    factors = [jnp.exp(maxima - top) for maxima, _ in found]
    total = sum(factor * sums for factor, (_, sums) in zip(factors, found))
    values = []
    for k in range(8):
        values.append(
            sum(
                piece[8 * k : 8 * k + 8, :].astype(F32) * spread(factor, k)
                for piece, factor in zip(pieces, factors)
            )
        )
    return top, total, values


def merge_kernel(*refs):
    out_ref = refs[-1]
    top, total, values = merged(refs[:-1])
    packed = pack_statistics(top, total)
    dense = jnp.concatenate(values, axis=0).astype(BF16)
    for copy in range(out_ref.shape[0]):
        out_ref[copy, :64, :] = dense
        out_ref[copy, 64:72, :] = packed


def finish_kernel(in_ref, weight_ref, out_ref, attended_ref):
    top, total, values = merged([in_ref.at[i] for i in range(in_ref.shape[0])])
    for k in range(8):
        attended_ref[8 * k : 8 * k + 8, :] = values[k] / spread(total, k)
    attended = jnp.concatenate(
        [attended_ref[pl.ds(k, 4, stride=16), :] for k in range(16)], axis=1
    ).astype(BF16)
    out_ref[...] = jnp.dot(attended, weight_ref[...], preferred_element_type=F32).astype(BF16)


def limit(mebibytes):
    return pltpu.CompilerParams(vmem_limit_bytes=mebibytes << 20)


def in_vmem(count):
    return [pl.BlockSpec(memory_space=VMEM)] * count


def in_hbm(count):
    return [pl.BlockSpec(memory_space=pltpu.HBM)] * count


def held(*arrays):
    return [pltpu.with_memory_space_constraint(array, pltpu.HBM) for array in arrays]


def exchanged(array, axis):
    return lax.all_to_all(array, axis, 0, 0, tiled=True)


def with_peers(array, axis):
    size = lax.axis_size(axis)
    turns = [[(i, (i + k) % size) for i in range(size)] for k in range(1, size)]
    return [array] + [lax.ppermute(array, axis, turn) for turn in turns]


def per_device(
    tokens,
    norm_gain,
    query_weight,
    key_weight,
    value_weight,
    gate_weight,
    gate_bias,
    query_gain,
    key_gain,
    key_cache,
    value_cache,
    gate_cache,
    lengths,
    out_weight,
):
    seqs, columns = tokens.shape
    outer, inner = lax.axis_size("kv_0"), lax.axis_size("kv_1")
    sums, small = pl.pallas_call(
        project_kernel,
        out_shape=(
            jax.ShapeDtypeStruct((8, 1408), BF16),
            jax.ShapeDtypeStruct((8, 128), F32),
        ),
        in_specs=in_hbm(10),
        out_specs=tuple(in_vmem(2)),
        scratch_shapes=[
            VMEM(tokens.shape, BF16),
            VMEM((1, columns), F32),
            VMEM(query_weight.shape, BF16),
            VMEM(key_weight.shape, BF16),
            VMEM(value_weight.shape, BF16),
            VMEM((KV_HEADS, columns), BF16),
            VMEM((1, KV_HEADS), F32),
            VMEM((1, HEAD), F32),
            VMEM((1, HEAD), F32),
            VMEM((1, seqs), jnp.int32),
            pltpu.SemaphoreType.DMA((10,)),
        ],
        compiler_params=limit(4),
        name="project",
    )(
        *held(
            tokens,
            norm_gain[None],
            query_weight,
            key_weight,
            value_weight,
            gate_weight.T,
            gate_bias[None],
            query_gain[None],
            key_gain[None],
            lengths[None],
        )
    )
    sums = pl.pallas_call(
        fold_kernel,
        out_shape=jax.ShapeDtypeStruct((outer, 8, 1408), BF16),
        in_specs=in_vmem(inner),
        out_specs=in_vmem(1)[0],
        compiler_params=limit(4),
        cost_estimate=pl.CostEstimate(
            flops=10**10, bytes_accessed=10**8, transcendentals=0
        ),
        name="fold",
    )(*with_peers(sums, "kv_1"))
    parts = pl.pallas_call(
        attend_kernel,
        out_shape=jax.ShapeDtypeStruct((72, 128), BF16),
        in_specs=in_vmem(5),
        out_specs=in_vmem(1)[0],
        scratch_shapes=[
            VMEM((64, 128), F32),
            VMEM((32 * seqs, POSITIONS), F32),
            VMEM((32 * seqs, POSITIONS), BF16),
        ],
        compiler_params=limit(24),
        name="attend",
    )(exchanged(sums, "kv_0"), small, gate_cache, key_cache, value_cache)
    parts = pl.pallas_call(
        merge_kernel,
        out_shape=jax.ShapeDtypeStruct((outer, 72, 128), BF16),
        in_specs=in_vmem(inner),
        out_specs=in_vmem(1)[0],
        compiler_params=limit(4),
        name="merge",
    )(*with_peers(parts, "kv_1"))
    mixed = pl.pallas_call(
        finish_kernel,
        out_shape=jax.ShapeDtypeStruct((seqs, out_weight.shape[1]), BF16),
        in_specs=in_vmem(2),
        out_specs=in_vmem(1)[0],
        scratch_shapes=[VMEM((64, 128), F32)],
        compiler_params=limit(4),
        name="finish",
    )(exchanged(parts, "kv_0"), out_weight)
    other = lax.ppermute(mixed, "tp", [(0, 1), (1, 0)])
    return (mixed.astype(F32) + other.astype(F32)).astype(BF16)


def solution(mesh):
    finer = Mesh(
        mesh.devices.reshape(mesh.shape["dp"], 8, 4, mesh.shape["tp"]), ("dp", "kv_0", "kv_1", "tp")
    )
    in_specs = (
        P("dp", KV),
        P(KV),
        P(KV, "tp"),
        P(KV, "tp"),
        P(KV, "tp"),
        P(),
        P(),
        P(),
        P(),
        P("dp", KV, "tp"),
        P("dp", KV, "tp"),
        P("dp", "tp", KV),
        P("dp"),
        P("tp", KV),
    )
    out_specs = P("dp", KV)
    return jax.shard_map(
        per_device, mesh=finer, in_specs=in_specs, out_specs=out_specs, check_vma=False
    )
```

```python
import functools

import jax
import jax.numpy as jnp
from jax import lax
from jax.experimental import pallas as pl
from jax.experimental.pallas import tpu as pltpu
from jax.sharding import Mesh
from jax.sharding import PartitionSpec as P

D = 4096
HEADS = 64
KV_HEADS = 8
HEAD = 64
POSITIONS = 2048
KV = ("kv_0", "kv_1")


EPSILON = 1e-06
FLOOR = -1e30
VMEM = pltpu.VMEM
F32 = jnp.float32
BF16 = jnp.bfloat16


def lanes_of(shape):
    return lax.broadcasted_iota(jnp.int32, shape, 1)


def halves_stacked(part):
    half = part.shape[1] // 2
    return jnp.concatenate([part[:, :half], part[:, half:]], axis=0)


def project_kernel(
    tokens_hbm,
    norm_gain_hbm,
    query_hbm,
    key_hbm,
    value_hbm,
    gate_hbm,
    bias_hbm,
    query_gain_hbm,
    key_gain_hbm,
    lengths_hbm,
    out_ref,
    small_ref,
    tokens_ref,
    norm_gain_ref,
    query_ref,
    key_ref,
    value_ref,
    gate_ref,
    bias_ref,
    query_gain_ref,
    key_gain_ref,
    lengths_ref,
    arrived,
):
    kv_rank = lax.axis_index(KV)
    columns = tokens_ref.shape[1]
    mine = pl.ds(pl.multiple_of(kv_rank * columns, columns), columns)
    pairs = [
        (tokens_hbm, tokens_ref),
        (norm_gain_hbm, norm_gain_ref),
        (query_hbm, query_ref),
        (key_hbm, key_ref),
        (value_hbm, value_ref),
        (gate_hbm.at[:, mine], gate_ref),
        (bias_hbm, bias_ref),
        (query_gain_hbm, query_gain_ref),
        (key_gain_hbm, key_gain_ref),
        (lengths_hbm, lengths_ref),
    ]
    copies = [pltpu.make_async_copy(*pair, arrived.at[k]) for k, pair in enumerate(pairs)]
    for copy in copies:
        copy.start()
    copies[0].wait()
    copies[1].wait()
    tokens = tokens_ref[...].astype(F32)
    squares = jnp.sum(tokens * tokens, axis=1, keepdims=True)
    scaled = (tokens * norm_gain_ref[...]).astype(BF16)
    for copy in copies[2:]:
        copy.wait()
    query = jnp.dot(scaled, query_ref[...], preferred_element_type=F32)
    key = jnp.dot(scaled, key_ref[...], preferred_element_type=F32)
    value = jnp.dot(scaled, value_ref[...], preferred_element_type=F32)
    rows = jnp.concatenate([gate_ref[...].astype(F32), jnp.zeros((120, 128), F32)], axis=0)
    gate = lax.dot_general(
        scaled, rows.astype(BF16), (((1,), (1,)), ((), ())), preferred_element_type=F32
    )
    extra = jnp.concatenate([jnp.broadcast_to(squares, gate.shape), gate], axis=0)
    whole = jnp.concatenate(
        [halves_stacked(query), halves_stacked(key), halves_stacked(value), extra], axis=1
    ).astype(BF16)
    out_ref[...] = whole
    small_ref[0:1, :] = jnp.concatenate([query_gain_ref[...]] * 2, axis=1)
    small_ref[1:2, :] = jnp.concatenate([key_gain_ref[...]] * 2, axis=1)
    small_ref[2:3, :] = jnp.zeros((1, 128), F32)
    small_ref[2:3, 0 : bias_ref.shape[1]] = bias_ref[...]
    rest = lengths_ref[...] - kv_rank * POSITIONS
    small_ref[3:4, :] = jnp.zeros((1, 128), F32)
    small_ref[3:4, 0 : rest.shape[1]] = rest.astype(F32)


def fold_kernel(*refs):
    out_ref = refs[-1]
    total = sum(ref[...].astype(F32) for ref in refs[:-1]).astype(BF16)
    for copy in range(out_ref.shape[0]):
        out_ref[copy] = total


def attend_kernel(
    sums_ref,
    small_ref,
    gate_ref,
    key_ref,
    value_ref,
    out_ref,
    query_ref,
    scores_ref,
    weights_ref,
):
    tp_rank = lax.axis_index("tp")
    seqs, positions = gate_ref.shape[0], gate_ref.shape[2]
    total = sums_ref[0].astype(F32)
    for piece in range(1, sums_ref.shape[0]):
        total = total + sums_ref[piece].astype(F32)
    extra = total[:, 1280:]
    inverse = lax.rsqrt(extra[:seqs] / D + EPSILON)
    logit = extra[seqs:] * inverse + small_ref[2:3, :]
    log_gate = jnp.minimum(logit, 0.0) - jnp.log1p(jnp.exp(-jnp.abs(logit)))
    inverse = jnp.concatenate([inverse, inverse], axis=0)
    tiles = [
        (total[:, 128 * k : 128 * (k + 1)] * inverse).astype(BF16).astype(F32) for k in range(10)
    ]
    for k in range(8):
        query_ref[8 * k : 8 * k + 8, :] = tiles[k]

    def normed(part, gain):
        mean = jnp.sum(part * part, axis=1, keepdims=True) * (1.0 / HEAD)
        return (part * lax.rsqrt(mean + EPSILON) * gain).astype(BF16).astype(F32)

    query_gain, key_gain = small_ref[0:1, :], small_ref[1:2, :]
    lane = lanes_of((8, 128))
    left = lane < HEAD
    early = lax.broadcasted_iota(jnp.int32, (8, 128), 0) < 4
    blocks = positions // 128
    rest = [
        jnp.broadcast_to(small_ref[3:4, s : s + 1], (8, 128)).astype(jnp.int32)
        for s in range(seqs)
    ]
    owner = [jnp.logical_and(r >= 1, r <= positions) for r in rest]

    def gate_rows(s, a, j):
        part = slice(128 * j, 128 * j + 128)
        return jnp.where(
            early, gate_ref[s, 2 * a : 2 * a + 1, part], gate_ref[s, 2 * a + 1 : 2 * a + 2, part]
        )

    placed = left == early
    keys_new = normed(jnp.where(left, tiles[8], 0.0), key_gain)
    keys_new = keys_new + normed(jnp.where(left, 0.0, tiles[8]), key_gain)
    values_new = tiles[9]
    parts = {}
    for s in range(seqs):
        for a in range(2):
            heads = query_ref[pl.ds(a * seqs + s, 8, stride=8), :]
            turned = pltpu.roll(heads, HEAD, 1)
            for p, part in enumerate((heads, turned)):
                part = normed(jnp.where(placed, part, 0.0), query_gain)
                parts[s, a, p] = part * HEAD ** (-0.5)
    zeros = jnp.zeros((16, 128), F32)
    for s in range(seqs):
        query = jnp.concatenate(
            [
                jnp.concatenate([parts[s, 0, 0], parts[s, 0, 1], zeros], axis=0),
                jnp.concatenate([zeros, parts[s, 1, 0], parts[s, 1, 1]], axis=0),
            ],
            axis=1,
        ).astype(BF16)
        scores_ref[32 * s : 32 * s + 32, :] = lax.dot_general(
            query, key_ref[s], (((1,), (1,)), ((), ())), preferred_element_type=F32
        )

    tops, owns = {}, {}
    for s in range(seqs):
        for a in range(2):
            tops[s, a, 0] = tops[s, a, 1] = jnp.full((8, 128), FLOOR, F32)
            owns[s, a] = jnp.zeros((8, 128), F32)
        for j in range(blocks):
            place = lane + 128 * j
            live, last = place < rest[s], place == rest[s] - 1
            for a in range(2):
                gate = gate_rows(s, a, j)
                owns[s, a] = owns[s, a] + jnp.where(last, gate, 0.0)
                for p in range(2):
                    at = 32 * s + 16 * a + 8 * p
                    score = scores_ref[at : at + 8, 128 * j : 128 * j + 128] - gate
                    score = jnp.where(live, score, FLOOR)
                    scores_ref[at : at + 8, 128 * j : 128 * j + 128] = score
                    tops[s, a, p] = jnp.maximum(tops[s, a, p], score)
    rows = [(s, a, p) for s in range(seqs) for a in range(2) for p in range(2)]
    fresh, top, weight_new = {}, {}, {}
    for s in range(seqs):
        for a in range(2):
            wanted = jnp.where(early, 2 * a, 2 * a + 1) + tp_rank * (KV_HEADS // 2)
            own = owns[s, a] + jnp.where(lane == wanted, log_gate[s : s + 1, :], 0.0)
            key_new = keys_new[a * seqs + s : a * seqs + s + 1, :]
            for p in range(2):
                fresh[s, a, p] = jnp.sum(parts[s, a, p] * key_new - own, axis=1, keepdims=True)
    for s, a, p in rows:
        most = jnp.max(tops[s, a, p], axis=1, keepdims=True)
        new = jnp.broadcast_to(fresh[s, a, p], (8, 128))
        most = jnp.broadcast_to(most, (8, 128))
        top[s, a, p] = jnp.where(owner[s], jnp.maximum(most, new), most)
        weight = jnp.where(owner[s], jnp.exp(new - top[s, a, p]), 0.0)
        weight_new[s, a, p] = weight.astype(BF16).astype(F32)
    counts = {}
    for s in range(seqs):
        for a in range(2):
            counts[s, a, 0] = counts[s, a, 1] = jnp.zeros((8, 128), F32)
        for j in range(blocks):
            live = lane + 128 * j < rest[s]
            for a in range(2):
                both = []
                for p in range(2):
                    at = 32 * s + 16 * a + 8 * p
                    score = scores_ref[at : at + 8, 128 * j : 128 * j + 128]
                    weight = jnp.where(live, jnp.exp(score - top[s, a, p]), 0.0).astype(BF16)
                    counts[s, a, p] = counts[s, a, p] + weight.astype(F32)
                    both.append(weight)
                at = 32 * s + 16 * a
                weights_ref[at : at + 16, 128 * j : 128 * j + 128] = jnp.concatenate(both, axis=0)
    summed = [
        jnp.dot(
            weights_ref[32 * s : 32 * s + 32, :], value_ref[s], preferred_element_type=F32
        )
        for s in range(seqs)
    ]
    maxima = jnp.zeros((8, 128), F32)
    sums = jnp.zeros((8, 128), F32)
    for s, a, p in rows:
        here = lane == 4 * s + 2 * a + jnp.where(early, p, 1 - p)
        count = jnp.sum(counts[s, a, p], axis=1, keepdims=True) + weight_new[s, a, p]
        maxima = jnp.where(here, top[s, a, p], maxima)
        sums = jnp.where(here, count, sums)
    packed = pack_statistics(maxima, sums)
    for s in range(seqs):
        for a in range(2):
            new = values_new[a * seqs + s : a * seqs + s + 1, :]
            even, odd = (
                summed[s][16 * a + 8 * p : 16 * a + 8 * p + 8, 128 * a : 128 * a + 128]
                + weight_new[s, a, p] * new
                for p in range(2)
            )
            dense = jnp.where(placed, even, pltpu.roll(odd, HEAD, 1)).astype(BF16)
            at = 8 * (2 * s + a)
            out_ref[at : at + 8, :] = dense
    out_ref[64:72, :] = packed


def pack_statistics(maxima, sums):
    first = maxima.astype(BF16).astype(F32)
    second = (maxima - first).astype(BF16).astype(F32)
    third = (maxima - first - second).astype(BF16).astype(F32)
    high = sums.astype(BF16).astype(F32)
    low = (sums - high).astype(BF16).astype(F32)
    packed = first + pltpu.roll(second, 16, 1) + pltpu.roll(third, 32, 1)
    packed = packed + pltpu.roll(high, 48, 1) + pltpu.roll(low, 64, 1)
    return packed.astype(BF16)


def unpack_statistics(packed):
    packed = packed.astype(F32)
    valid = lanes_of((8, 128)) < 16
    maxima = packed + pltpu.roll(packed, 112, 1) + pltpu.roll(packed, 96, 1)
    sums = pltpu.roll(packed, 80, 1) + pltpu.roll(packed, 64, 1)
    return jnp.where(valid, maxima, 0.0), jnp.where(valid, sums, 0.0)


def spread(tile, k):
    left = lanes_of((8, 128)) < HEAD
    return jnp.where(left, tile[:, 2 * k : 2 * k + 1], tile[:, 2 * k + 1 : 2 * k + 2])


def merged(pieces, divide):
    found = [unpack_statistics(piece[64:72, :]) for piece in pieces]
    top = functools.reduce(jnp.maximum, [maxima for maxima, _ in found])
    factors = [jnp.exp(maxima - top) for maxima, _ in found]
    total = sum(factor * sums for factor, (_, sums) in zip(factors, found))
    if divide:
        share = 1.0 / jnp.where(lanes_of((8, 128)) < 16, total, 1.0)
        factors = [factor * share for factor in factors]
    values = []
    for k in range(8):
        values.append(
            sum(
                piece[8 * k : 8 * k + 8, :].astype(F32) * spread(factor, k)
                for piece, factor in zip(pieces, factors)
            )
        )
    return top, total, values


def merge_kernel(*refs):
    out_ref = refs[-1]
    top, total, values = merged(refs[:-1], False)
    packed = pack_statistics(top, total)
    dense = jnp.concatenate(values, axis=0).astype(BF16)
    for copy in range(out_ref.shape[0]):
        out_ref[copy, :64, :] = dense
        out_ref[copy, 64:72, :] = packed


def finish_kernel(in_ref, weight_ref, out_ref, attended_ref):
    values = merged([in_ref.at[i] for i in range(in_ref.shape[0])], True)[2]
    for k in range(8):
        attended_ref[8 * k : 8 * k + 8, :] = values[k]
    attended = jnp.concatenate(
        [attended_ref[pl.ds(k, 4, stride=16), :] for k in range(16)], axis=1
    ).astype(BF16)
    out_ref[...] = jnp.dot(attended, weight_ref[...], preferred_element_type=F32).astype(BF16)


def limit(mebibytes):
    return pltpu.CompilerParams(vmem_limit_bytes=mebibytes << 20)


def in_vmem(count):
    return [pl.BlockSpec(memory_space=VMEM)] * count


def in_hbm(count):
    return [pl.BlockSpec(memory_space=pltpu.HBM)] * count


def held(*arrays):
    return [pltpu.with_memory_space_constraint(array, pltpu.HBM) for array in arrays]


def exchanged(array, axis):
    return lax.all_to_all(array, axis, 0, 0, tiled=True)


def with_peers(array, axis):
    size = lax.axis_size(axis)
    pairs = [[(i, i ^ k) for i in range(size)] for k in range(1, size)]
    return [array] + [lax.ppermute(array, axis, pair) for pair in pairs]


def per_device(
    tokens,
    norm_gain,
    query_weight,
    key_weight,
    value_weight,
    gate_weight,
    gate_bias,
    query_gain,
    key_gain,
    key_cache,
    value_cache,
    gate_cache,
    lengths,
    out_weight,
):
    seqs, columns = tokens.shape
    outer, inner = lax.axis_size("kv_0"), lax.axis_size("kv_1")
    sums, small = pl.pallas_call(
        project_kernel,
        out_shape=(
            jax.ShapeDtypeStruct((8, 1408), BF16),
            jax.ShapeDtypeStruct((8, 128), F32),
        ),
        in_specs=in_hbm(10),
        out_specs=tuple(in_vmem(2)),
        scratch_shapes=[
            VMEM(tokens.shape, BF16),
            VMEM((1, columns), F32),
            VMEM(query_weight.shape, BF16),
            VMEM(key_weight.shape, BF16),
            VMEM(value_weight.shape, BF16),
            VMEM((KV_HEADS, columns), BF16),
            VMEM((1, KV_HEADS), F32),
            VMEM((1, HEAD), F32),
            VMEM((1, HEAD), F32),
            VMEM((1, seqs), jnp.int32),
            pltpu.SemaphoreType.DMA((10,)),
        ],
        compiler_params=limit(4),
        name="project",
    )(
        *held(
            tokens,
            norm_gain[None],
            query_weight,
            key_weight,
            value_weight,
            gate_weight.T,
            gate_bias[None],
            query_gain[None],
            key_gain[None],
            lengths[None],
        )
    )
    sums = pl.pallas_call(
        fold_kernel,
        out_shape=jax.ShapeDtypeStruct((outer, 8, 1408), BF16),
        in_specs=in_vmem(inner),
        out_specs=in_vmem(1)[0],
        compiler_params=limit(4),
        cost_estimate=pl.CostEstimate(
            flops=10**10, bytes_accessed=10**8, transcendentals=0
        ),
        name="fold",
    )(*with_peers(sums, "kv_1"))
    parts = pl.pallas_call(
        attend_kernel,
        out_shape=jax.ShapeDtypeStruct((72, 128), BF16),
        in_specs=in_vmem(5),
        out_specs=in_vmem(1)[0],
        scratch_shapes=[
            VMEM((64, 128), F32),
            VMEM((32 * seqs, POSITIONS), F32),
            VMEM((32 * seqs, POSITIONS), BF16),
        ],
        compiler_params=limit(24),
        name="attend",
    )(exchanged(sums, "kv_0"), small, gate_cache, key_cache, value_cache)
    parts = pl.pallas_call(
        merge_kernel,
        out_shape=jax.ShapeDtypeStruct((outer, 72, 128), BF16),
        in_specs=in_vmem(inner),
        out_specs=in_vmem(1)[0],
        compiler_params=limit(4),
        name="merge",
    )(*with_peers(parts, "kv_1"))
    mixed = pl.pallas_call(
        finish_kernel,
        out_shape=jax.ShapeDtypeStruct((seqs, out_weight.shape[1]), BF16),
        in_specs=in_vmem(2),
        out_specs=in_vmem(1)[0],
        scratch_shapes=[VMEM((64, 128), F32)],
        compiler_params=limit(4),
        name="finish",
    )(exchanged(parts, "kv_0"), out_weight)
    other = lax.ppermute(mixed, "tp", [(0, 1), (1, 0)])
    return (mixed.astype(F32) + other.astype(F32)).astype(BF16)


def solution(mesh):
    finer = Mesh(
        mesh.devices.reshape(mesh.shape["dp"], 8, 4, mesh.shape["tp"]), ("dp", "kv_0", "kv_1", "tp")
    )
    in_specs = (
        P("dp", KV),
        P(KV),
        P(KV, "tp"),
        P(KV, "tp"),
        P(KV, "tp"),
        P(),
        P(),
        P(),
        P(),
        P("dp", KV, "tp"),
        P("dp", KV, "tp"),
        P("dp", "tp", KV),
        P("dp"),
        P("tp", KV),
    )
    out_specs = P("dp", KV)
    return jax.shard_map(
        per_device, mesh=finer, in_specs=in_specs, out_specs=out_specs, check_vma=False
    )
```

```python
import functools

import jax
import jax.numpy as jnp
from jax import lax
from jax.experimental import pallas as pl
from jax.experimental.pallas import tpu as pltpu
from jax.sharding import Mesh
from jax.sharding import PartitionSpec as P

D = 4096
HEADS = 64
KV_HEADS = 8
HEAD = 64
POSITIONS = 2048
PIECES = 1
KV = ("kv_0", "kv_1")


EPSILON = 1e-06
FLOOR = -1e30
VMEM = pltpu.VMEM
F32 = jnp.float32
BF16 = jnp.bfloat16


def lanes_of(shape):
    return lax.broadcasted_iota(jnp.int32, shape, 1)


def halves_stacked(part):
    half = part.shape[1] // 2
    return jnp.concatenate([part[:, :half], part[:, half:]], axis=0)


def project_kernel(
    tokens_hbm,
    norm_gain_hbm,
    query_hbm,
    key_hbm,
    value_hbm,
    gate_hbm,
    out_ref,
    tokens_ref,
    norm_gain_ref,
    query_ref,
    key_ref,
    value_ref,
    gate_ref,
    arrived,
):
    seqs, columns = tokens_ref.shape
    kv_rank = lax.axis_index(KV)
    mine = pl.ds(pl.multiple_of(kv_rank * columns, columns), columns)
    pairs = [(tokens_hbm, tokens_ref), (norm_gain_hbm, norm_gain_ref)]
    step = columns // PIECES
    for k in range(PIECES):
        rows = slice(step * k, step * k + step)
        pairs.append((query_hbm.at[rows, :], query_ref.at[rows, :]))
    pairs += [
        (key_hbm, key_ref),
        (value_hbm, value_ref),
        (gate_hbm.at[:, mine], gate_ref),
    ]
    copies = [pltpu.make_async_copy(*pair, arrived.at[k]) for k, pair in enumerate(pairs)]
    for copy in copies:
        copy.start()
    for copy in copies[:2]:
        copy.wait()
    tokens = tokens_ref[...].astype(F32)
    squares = jnp.sum(tokens * tokens, axis=1, keepdims=True)
    scaled = (tokens * norm_gain_ref[...]).astype(BF16)
    for copy in copies[2:]:
        copy.wait()
    query = jnp.dot(scaled, query_ref[...], preferred_element_type=F32)
    key = jnp.dot(scaled, key_ref[...], preferred_element_type=F32)
    value = jnp.dot(scaled, value_ref[...], preferred_element_type=F32)
    rows = gate_ref[...].astype(F32)
    rows = jnp.concatenate([rows, jnp.zeros((128 - KV_HEADS, columns), F32)], axis=0)
    gate = lax.dot_general(
        scaled, rows.astype(BF16), (((1,), (1,)), ((), ())), preferred_element_type=F32
    )
    extra = jnp.concatenate([jnp.broadcast_to(squares, gate.shape), gate], axis=0)
    out_ref[...] = jnp.concatenate(
        [halves_stacked(query), extra, halves_stacked(key), halves_stacked(value)], axis=1
    ).astype(BF16)


def relay_kernel(in_ref, out_ref):
    out_ref[...] = in_ref[...]


def prepare_kernel(
    bias_hbm,
    query_gain_hbm,
    key_gain_hbm,
    lengths_hbm,
    cache_hbm,
    keys_ref,
    small_ref,
    turned_ref,
    bias_ref,
    query_gain_ref,
    key_gain_ref,
    lengths_ref,
    cache_ref,
    arrived,
):
    pairs = [
        (bias_hbm, bias_ref),
        (query_gain_hbm, query_gain_ref),
        (key_gain_hbm, key_gain_ref),
        (lengths_hbm, lengths_ref),
        (cache_hbm, cache_ref),
    ]
    copies = [pltpu.make_async_copy(*pair, arrived.at[k]) for k, pair in enumerate(pairs)]
    for copy in copies:
        copy.start()
    for s in range(keys_ref.shape[0]):
        turned_ref[s] = keys_ref[s].T
    for copy in copies:
        copy.wait()
    seqs, groups, positions = cache_ref.shape
    small_ref[0:1, :] = jnp.concatenate([query_gain_ref[...]] * 2, axis=1)
    small_ref[1:2, :] = jnp.concatenate([key_gain_ref[...]] * 2, axis=1)
    small_ref[2:8, :] = jnp.zeros((6, 128), F32)
    small_ref[2:3, 0:KV_HEADS] = bias_ref[...]
    lengths = lengths_ref[...]
    rest = lengths - lax.axis_index(KV) * positions
    small_ref[3:4, 0:seqs] = rest.astype(F32)
    small_ref[3:4, seqs : 2 * seqs] = (
        ((lengths - 1) // positions) % lax.axis_size("kv_1")
    ).astype(F32)
    lane = lanes_of((groups, 128))
    row = lax.broadcasted_iota(jnp.int32, (groups, 128), 0)
    place = lanes_of((groups, positions))
    for s in range(seqs):
        last = jnp.where(place == rest[0:1, s : s + 1] - 1, cache_ref[s], 0.0)
        last = jnp.sum(last, axis=1, keepdims=True)
        gate = jnp.zeros((groups, 128), F32)
        for k in range(3):
            part = last.astype(BF16).astype(F32)
            last = last - part
            gate = gate + jnp.where(lane == KV_HEADS + groups * k + row, part, 0.0)
        small_ref[4 + s : 5 + s, :] = jnp.sum(gate, axis=0, keepdims=True)


def fold_kernel(*refs):
    *parts, small_ref, out_ref = refs
    total = sum(ref[...].astype(F32) for ref in parts)
    query = total[:, :1024].astype(BF16)
    extra, key, value = (total[:, 128 * k : 128 * k + 128] for k in (8, 9, 10))
    row = lax.broadcasted_iota(jnp.int32, (8, 128), 0)
    gates = extra[4:8] + small_ref[4:8, :]
    for z in range(out_ref.shape[0]):
        own = jnp.where(row == 5, value[z : z + 1], extra)
        own = jnp.where(row == 4, key[z : z + 1], own)
        own = jnp.where(row == 6, gates[z % 4 : z % 4 + 1], own)
        out_ref[z, :, :1024] = query
        out_ref[z, :, 1024:] = own.astype(BF16)


def attend_kernel(
    sums_ref,
    small_ref,
    gate_ref,
    key_ref,
    value_ref,
    out_ref,
    query_ref,
    scores_ref,
    weights_ref,
):
    tp_rank, z_rank = lax.axis_index("tp"), lax.axis_index("kv_0")
    x_rank = lax.axis_index("kv_1").astype(F32)
    seqs, positions = gate_ref.shape[0], gate_ref.shape[2]
    total = sums_ref[0].astype(F32)
    for piece in range(1, sums_ref.shape[0]):
        total = total + sums_ref[piece].astype(F32)
    extra = total[:, 1024:]
    inverse = lax.rsqrt(extra[:seqs] / D + EPSILON)
    both = jnp.concatenate([inverse, inverse], axis=0)
    for k in range(8):
        tile = total[:, 128 * k : 128 * k + 128] * both
        query_ref[8 * k : 8 * k + 8, :] = tile.astype(BF16).astype(F32)

    def normed(part, gain):
        mean = jnp.sum(part * part, axis=1, keepdims=True) * (1.0 / HEAD)
        return (part * lax.rsqrt(mean + EPSILON) * gain).astype(BF16).astype(F32)

    query_gain, key_gain = small_ref[0:1, :], small_ref[1:2, :]
    lane = lanes_of((8, 128))
    left = lane < HEAD
    early = lax.broadcasted_iota(jnp.int32, (8, 128), 0) < 4
    blocks = positions // 128
    rest = [
        jnp.broadcast_to(small_ref[3:4, s : s + 1], (8, 128)).astype(jnp.int32)
        for s in range(seqs)
    ]

    def gate_rows(s, a, j):
        part = slice(128 * j, 128 * j + 128)
        return jnp.where(
            early, gate_ref[s, 2 * a : 2 * a + 1, part], gate_ref[s, 2 * a + 1 : 2 * a + 2, part]
        )

    placed = left == early
    parts = {}
    for s in range(seqs):
        for a in range(2):
            heads = query_ref[pl.ds(a * seqs + s, 8, stride=8), :]
            turned = pltpu.roll(heads, HEAD, 1)
            for p, part in enumerate((heads, turned)):
                part = normed(jnp.where(placed, part, 0.0), query_gain)
                parts[s, a, p] = part * HEAD ** (-0.5)
    holds = [
        jnp.broadcast_to(small_ref[3:4, seqs + s : seqs + s + 1], (8, 128)) == x_rank
        for s in range(seqs)
    ]
    own_s, own_a = z_rank % seqs, z_rank // seqs
    scale = sum(jnp.where(own_s == s, inverse[s : s + 1], 0.0) for s in range(seqs))
    key_new = jnp.broadcast_to((extra[4:5] * scale).astype(BF16).astype(F32), (8, 128))
    value_new = (extra[5:6] * scale).astype(BF16).astype(F32)
    key_new = normed(jnp.where(left, key_new, 0.0), key_gain) + normed(
        jnp.where(left, 0.0, key_new), key_gain
    )
    logit = extra[6:7] * scale + small_ref[2:3, :]
    log_gate = jnp.minimum(logit, 0.0) - jnp.log1p(jnp.exp(-jnp.abs(logit)))
    group = jnp.where(early, 2 * own_a, 2 * own_a + 1)
    at = lane - group - KV_HEADS
    groups = KV_HEADS // 2
    last = jnp.logical_or(at == 0, jnp.logical_or(at == groups, at == 2 * groups))
    own = jnp.where(lane == group + groups * tp_rank, log_gate, 0.0) + jnp.where(
        last, extra[6:7], 0.0
    )
    joins = {
        (s, a): jnp.logical_and(holds[s], z_rank == seqs * a + s)
        for s in range(seqs)
        for a in range(2)
    }
    fresh = []
    for p in range(2):
        query = sum(
            jnp.where(z_rank == seqs * a + s, parts[s, a, p], 0.0)
            for s in range(seqs)
            for a in range(2)
        )
        fresh.append(jnp.sum(query * key_new - own, axis=1, keepdims=True))
    zeros = jnp.zeros((16, 128), F32)
    for s in range(seqs):
        query = jnp.concatenate(
            [
                jnp.concatenate([parts[s, 0, 0], parts[s, 0, 1], zeros], axis=0),
                jnp.concatenate([zeros, parts[s, 1, 0], parts[s, 1, 1]], axis=0),
            ],
            axis=1,
        ).astype(BF16)
        scores_ref[32 * s : 32 * s + 32, :] = lax.dot_general(
            query, key_ref[s], (((1,), (0,)), ((), ())), preferred_element_type=F32
        )

    tops = {}
    for s in range(seqs):
        for a in range(2):
            tops[s, a, 0] = tops[s, a, 1] = jnp.full((8, 128), FLOOR, F32)
        for j in range(blocks):
            live = lane + 128 * j < rest[s]
            for a in range(2):
                gate = gate_rows(s, a, j)
                for p in range(2):
                    at = 32 * s + 16 * a + 8 * p
                    score = scores_ref[at : at + 8, 128 * j : 128 * j + 128] - gate
                    score = jnp.where(live, score, FLOOR)
                    scores_ref[at : at + 8, 128 * j : 128 * j + 128] = score
                    tops[s, a, p] = jnp.maximum(tops[s, a, p], score)
    rows = [(s, a, p) for s in range(seqs) for a in range(2) for p in range(2)]
    top, weight_new = {}, {}
    for s, a, p in rows:
        most = jnp.max(tops[s, a, p], axis=1, keepdims=True)
        new = jnp.broadcast_to(fresh[p], (8, 128))
        most = jnp.broadcast_to(most, (8, 128))
        top[s, a, p] = jnp.where(joins[s, a], jnp.maximum(most, new), most)
        weight = jnp.where(joins[s, a], jnp.exp(new - top[s, a, p]), 0.0)
        weight_new[s, a, p] = weight.astype(BF16).astype(F32)
    counts = {}
    for s in range(seqs):
        for a in range(2):
            counts[s, a, 0] = counts[s, a, 1] = jnp.zeros((8, 128), F32)
        for j in range(blocks):
            live = lane + 128 * j < rest[s]
            for a in range(2):
                both = []
                for p in range(2):
                    at = 32 * s + 16 * a + 8 * p
                    score = scores_ref[at : at + 8, 128 * j : 128 * j + 128]
                    weight = jnp.where(live, jnp.exp(score - top[s, a, p]), 0.0).astype(BF16)
                    counts[s, a, p] = counts[s, a, p] + weight.astype(F32)
                    both.append(weight)
                at = 32 * s + 16 * a
                weights_ref[at : at + 16, 128 * j : 128 * j + 128] = jnp.concatenate(both, axis=0)
    summed = [
        jnp.dot(
            weights_ref[32 * s : 32 * s + 32, :], value_ref[s], preferred_element_type=F32
        )
        for s in range(seqs)
    ]
    maxima = jnp.zeros((8, 128), F32)
    sums = jnp.zeros((8, 128), F32)
    for s, a, p in rows:
        here = lane == 4 * s + 2 * a + jnp.where(early, p, 1 - p)
        count = jnp.sum(counts[s, a, p], axis=1, keepdims=True) + weight_new[s, a, p]
        maxima = jnp.where(here, top[s, a, p], maxima)
        sums = jnp.where(here, count, sums)
    packed = pack_statistics(maxima, sums)
    for s in range(seqs):
        for a in range(2):
            even, odd = (
                summed[s][16 * a + 8 * p : 16 * a + 8 * p + 8, 128 * a : 128 * a + 128]
                + weight_new[s, a, p] * value_new
                for p in range(2)
            )
            dense = jnp.where(placed, even, pltpu.roll(odd, HEAD, 1)).astype(BF16)
            at = 8 * (2 * s + a)
            out_ref[at : at + 8, :] = dense
    out_ref[64:72, :] = packed


def pack_statistics(maxima, sums):
    first = maxima.astype(BF16).astype(F32)
    second = (maxima - first).astype(BF16).astype(F32)
    third = (maxima - first - second).astype(BF16).astype(F32)
    high = sums.astype(BF16).astype(F32)
    low = (sums - high).astype(BF16).astype(F32)
    packed = first + pltpu.roll(second, 16, 1) + pltpu.roll(third, 32, 1)
    packed = packed + pltpu.roll(high, 48, 1) + pltpu.roll(low, 64, 1)
    return packed.astype(BF16)


def unpack_statistics(packed):
    packed = packed.astype(F32)
    valid = lanes_of((8, 128)) < 16
    maxima = packed + pltpu.roll(packed, 112, 1) + pltpu.roll(packed, 96, 1)
    sums = pltpu.roll(packed, 80, 1) + pltpu.roll(packed, 64, 1)
    return jnp.where(valid, maxima, 0.0), jnp.where(valid, sums, 0.0)


def spread(tile, k):
    left = lanes_of((8, 128)) < HEAD
    return jnp.where(left, tile[:, 2 * k : 2 * k + 1], tile[:, 2 * k + 1 : 2 * k + 2])


def merged(pieces, divide):
    found = [unpack_statistics(piece[64:72, :]) for piece in pieces]
    top = functools.reduce(jnp.maximum, [maxima for maxima, _ in found])
    factors = [jnp.exp(maxima - top) for maxima, _ in found]
    total = sum(factor * sums for factor, (_, sums) in zip(factors, found))
    if divide:
        share = 1.0 / jnp.where(lanes_of((8, 128)) < 16, total, 1.0)
        factors = [factor * share for factor in factors]
    values = []
    for k in range(8):
        values.append(
            sum(
                piece[8 * k : 8 * k + 8, :].astype(F32) * spread(factor, k)
                for piece, factor in zip(pieces, factors)
            )
        )
    return top, total, values


def merge_kernel(*refs):
    out_ref = refs[-1]
    top, total, values = merged(refs[:-1], False)
    packed = pack_statistics(top, total)
    dense = jnp.concatenate(values, axis=0).astype(BF16)
    for copy in range(out_ref.shape[0]):
        out_ref[copy, :64, :] = dense
        out_ref[copy, 64:72, :] = packed


def finish_kernel(in_ref, weight_ref, out_ref, attended_ref):
    values = merged([in_ref.at[i] for i in range(in_ref.shape[0])], True)[2]
    for k in range(8):
        attended_ref[8 * k : 8 * k + 8, :] = values[k]
    attended = jnp.concatenate(
        [attended_ref[pl.ds(k, 4, stride=16), :] for k in range(16)], axis=1
    ).astype(BF16)
    out_ref[...] = jnp.dot(attended, weight_ref[...], preferred_element_type=F32).astype(BF16)


def limit(mebibytes):
    return pltpu.CompilerParams(vmem_limit_bytes=mebibytes << 20)


def in_vmem(count):
    return [pl.BlockSpec(memory_space=VMEM)] * count


def in_hbm(count):
    return [pl.BlockSpec(memory_space=pltpu.HBM)] * count


def held(*arrays):
    return [pltpu.with_memory_space_constraint(array, pltpu.HBM) for array in arrays]


def exchanged(array, axis):
    return lax.all_to_all(array, axis, 0, 0, tiled=True)


def with_peers(array, axis):
    size = lax.axis_size(axis)
    pairs = [[(i, i ^ k) for i in range(size)] for k in range(1, size)]
    return [array] + [lax.ppermute(array, axis, pair) for pair in pairs]


def per_device(
    tokens,
    norm_gain,
    query_weight,
    key_weight,
    value_weight,
    gate_weight,
    gate_bias,
    query_gain,
    key_gain,
    key_cache,
    value_cache,
    gate_cache,
    lengths,
    out_weight,
):
    seqs, columns = tokens.shape
    outer, inner = lax.axis_size("kv_0"), lax.axis_size("kv_1")
    sums = pl.pallas_call(
        project_kernel,
        out_shape=jax.ShapeDtypeStruct((8, 1408), BF16),
        in_specs=in_hbm(6),
        out_specs=in_vmem(1)[0],
        scratch_shapes=[
            VMEM(tokens.shape, BF16),
            VMEM((1, columns), F32),
            VMEM(query_weight.shape, BF16),
            VMEM(key_weight.shape, BF16),
            VMEM(value_weight.shape, BF16),
            VMEM((KV_HEADS, columns), BF16),
            pltpu.SemaphoreType.DMA((5 + PIECES,)),
        ],
        compiler_params=limit(4),
        name="project",
    )(
        *held(
            tokens, norm_gain[None], query_weight, key_weight, value_weight, gate_weight.T
        )
    )
    sums = pl.pallas_call(
        relay_kernel,
        out_shape=jax.ShapeDtypeStruct((8, 1408), BF16),
        in_specs=in_vmem(1),
        out_specs=in_vmem(1)[0],
        compiler_params=limit(4),
        cost_estimate=pl.CostEstimate(
            flops=10**10, bytes_accessed=10**8, transcendentals=0
        ),
        name="relay",
    )(sums)
    small, keys = pl.pallas_call(
        prepare_kernel,
        out_shape=(
            jax.ShapeDtypeStruct((8, 128), F32),
            jax.ShapeDtypeStruct((seqs, key_cache.shape[2], POSITIONS), BF16),
        ),
        in_specs=in_hbm(5) + in_vmem(1),
        out_specs=tuple(in_vmem(2)),
        scratch_shapes=[
            VMEM((1, KV_HEADS), F32),
            VMEM((1, HEAD), F32),
            VMEM((1, HEAD), F32),
            VMEM((1, seqs), jnp.int32),
            VMEM(gate_cache.shape, F32),
            pltpu.SemaphoreType.DMA((5,)),
        ],
        compiler_params=limit(16),
        cost_estimate=pl.CostEstimate(flops=10**9, bytes_accessed=10**7, transcendentals=0),
        name="prepare",
    )(
        *held(gate_bias[None], query_gain[None], key_gain[None], lengths[None], gate_cache),
        key_cache,
    )
    received, small, keys = lax.optimization_barrier((with_peers(sums, "kv_1"), small, keys))
    sums = pl.pallas_call(
        fold_kernel,
        out_shape=jax.ShapeDtypeStruct((outer, 8, 1152), BF16),
        in_specs=in_vmem(inner + 1),
        out_specs=in_vmem(1)[0],
        compiler_params=limit(4),
        cost_estimate=pl.CostEstimate(
            flops=10**10, bytes_accessed=10**8, transcendentals=0
        ),
        name="fold",
    )(*received, small)
    parts = pl.pallas_call(
        attend_kernel,
        out_shape=jax.ShapeDtypeStruct((72, 128), BF16),
        in_specs=in_vmem(5),
        out_specs=in_vmem(1)[0],
        scratch_shapes=[
            VMEM((64, 128), F32),
            VMEM((32 * seqs, POSITIONS), F32),
            VMEM((32 * seqs, POSITIONS), BF16),
        ],
        compiler_params=limit(24),
        name="attend",
    )(exchanged(sums, "kv_0"), small, gate_cache, keys, value_cache)
    parts = pl.pallas_call(
        merge_kernel,
        out_shape=jax.ShapeDtypeStruct((outer, 72, 128), BF16),
        in_specs=in_vmem(inner),
        out_specs=in_vmem(1)[0],
        compiler_params=limit(4),
        name="merge",
    )(*with_peers(parts, "kv_1"))
    mixed = pl.pallas_call(
        finish_kernel,
        out_shape=jax.ShapeDtypeStruct((seqs, out_weight.shape[1]), BF16),
        in_specs=in_vmem(2),
        out_specs=in_vmem(1)[0],
        scratch_shapes=[VMEM((64, 128), F32)],
        compiler_params=limit(4),
        name="finish",
    )(exchanged(parts, "kv_0"), out_weight)
    other = lax.ppermute(mixed, "tp", [(0, 1), (1, 0)])
    return (mixed.astype(F32) + other.astype(F32)).astype(BF16)


def solution(mesh):
    finer = Mesh(
        mesh.devices.reshape(mesh.shape["dp"], 8, 4, mesh.shape["tp"]), ("dp", "kv_0", "kv_1", "tp")
    )
    in_specs = (
        P("dp", KV),
        P(KV),
        P(KV, "tp"),
        P(KV, "tp"),
        P(KV, "tp"),
        P(),
        P(),
        P(),
        P(),
        P("dp", KV, "tp"),
        P("dp", KV, "tp"),
        P("dp", "tp", KV),
        P("dp"),
        P("tp", KV),
    )
    out_specs = P("dp", KV)
    return jax.shard_map(
        per_device, mesh=finer, in_specs=in_specs, out_specs=out_specs, check_vma=False
    )
```

```python
import functools

import jax
import jax.numpy as jnp
from jax import lax
from jax.experimental import pallas as pl
from jax.experimental.pallas import tpu as pltpu
from jax.sharding import Mesh
from jax.sharding import PartitionSpec as P

D = 4096
HEADS = 64
KV_HEADS = 8
HEAD = 64
POSITIONS = 2048
PIECES = 1
KV = ("kv_0", "kv_1")


EPSILON = 1e-06
FLOOR = -1e30
VMEM = pltpu.VMEM
F32 = jnp.float32
BF16 = jnp.bfloat16


def lanes_of(shape):
    return lax.broadcasted_iota(jnp.int32, shape, 1)


def halves_stacked(part):
    half = part.shape[1] // 2
    return jnp.concatenate([part[:, :half], part[:, half:]], axis=0)


def project_kernel(
    tokens_hbm,
    norm_gain_hbm,
    query_hbm,
    key_hbm,
    value_hbm,
    gate_hbm,
    out_ref,
    tokens_ref,
    norm_gain_ref,
    query_ref,
    key_ref,
    value_ref,
    gate_ref,
    arrived,
):
    seqs, columns = tokens_ref.shape
    kv_rank = lax.axis_index(KV)
    mine = pl.ds(pl.multiple_of(kv_rank * columns, columns), columns)
    pairs = [(tokens_hbm, tokens_ref), (norm_gain_hbm, norm_gain_ref)]
    step = columns // PIECES
    for k in range(PIECES):
        rows = slice(step * k, step * k + step)
        pairs.append((query_hbm.at[rows, :], query_ref.at[rows, :]))
    pairs += [
        (key_hbm, key_ref),
        (value_hbm, value_ref),
        (gate_hbm.at[:, mine], gate_ref),
    ]
    copies = [pltpu.make_async_copy(*pair, arrived.at[k]) for k, pair in enumerate(pairs)]
    for copy in copies:
        copy.start()
    for copy in copies[:2]:
        copy.wait()
    tokens = tokens_ref[...].astype(F32)
    squares = jnp.sum(tokens * tokens, axis=1, keepdims=True)
    scaled = (tokens * norm_gain_ref[...]).astype(BF16)
    for copy in copies[2:]:
        copy.wait()
    query = jnp.dot(scaled, query_ref[...], preferred_element_type=F32)
    key = jnp.dot(scaled, key_ref[...], preferred_element_type=F32)
    value = jnp.dot(scaled, value_ref[...], preferred_element_type=F32)
    rows = gate_ref[...].astype(F32)
    rows = jnp.concatenate([rows, jnp.zeros((128 - KV_HEADS, columns), F32)], axis=0)
    gate = lax.dot_general(
        scaled, rows.astype(BF16), (((1,), (1,)), ((), ())), preferred_element_type=F32
    )
    extra = jnp.concatenate([jnp.broadcast_to(squares, gate.shape), gate], axis=0)
    out_ref[...] = jnp.concatenate(
        [halves_stacked(query), extra, halves_stacked(key), halves_stacked(value)], axis=1
    ).astype(BF16)


def relay_kernel(in_ref, out_ref):
    out_ref[...] = in_ref[...]


def prepare_kernel(
    bias_hbm,
    query_gain_hbm,
    key_gain_hbm,
    lengths_hbm,
    cache_hbm,
    keys_ref,
    small_ref,
    turned_ref,
    gates_ref,
    bias_ref,
    query_gain_ref,
    key_gain_ref,
    lengths_ref,
    cache_ref,
    arrived,
):
    pairs = [
        (bias_hbm, bias_ref),
        (query_gain_hbm, query_gain_ref),
        (key_gain_hbm, key_gain_ref),
        (lengths_hbm, lengths_ref),
        (cache_hbm, cache_ref),
    ]
    copies = [pltpu.make_async_copy(*pair, arrived.at[k]) for k, pair in enumerate(pairs)]
    for copy in copies:
        copy.start()
    for s in range(keys_ref.shape[0]):
        turned_ref[s] = keys_ref[s].T
    for copy in copies:
        copy.wait()
    seqs, groups, positions = cache_ref.shape
    small_ref[0:1, :] = jnp.concatenate([query_gain_ref[...]] * 2, axis=1)
    small_ref[1:2, :] = jnp.concatenate([key_gain_ref[...]] * 2, axis=1)
    small_ref[2:8, :] = jnp.zeros((6, 128), F32)
    small_ref[2:3, 0:KV_HEADS] = bias_ref[...]
    lengths = lengths_ref[...]
    rest = lengths - lax.axis_index(KV) * positions
    small_ref[3:4, 0:seqs] = rest.astype(F32)
    small_ref[3:4, seqs : 2 * seqs] = (
        ((lengths - 1) // positions) % lax.axis_size("kv_1")
    ).astype(F32)
    lane, blocks = lanes_of((8, 128)), positions // 128
    early = lax.broadcasted_iota(jnp.int32, (8, 128), 0) < 4
    for s in range(seqs):
        left = jnp.broadcast_to(rest[0:1, s : s + 1], (8, 128))
        for j in range(blocks):
            part = slice(128 * j, 128 * j + 128)
            live = lane + 128 * j < left
            for a in range(2):
                gate = jnp.where(
                    early,
                    cache_ref[s, 2 * a : 2 * a + 1, part],
                    cache_ref[s, 2 * a + 1 : 2 * a + 2, part],
                )
                gates_ref[s, 8 * a : 8 * a + 8, part] = jnp.where(live, gate, -FLOOR)
    lane = lanes_of((groups, 128))
    row = lax.broadcasted_iota(jnp.int32, (groups, 128), 0)
    place = lanes_of((groups, positions))
    for s in range(seqs):
        last = jnp.where(place == rest[0:1, s : s + 1] - 1, cache_ref[s], 0.0)
        last = jnp.sum(last, axis=1, keepdims=True)
        gate = jnp.zeros((groups, 128), F32)
        for k in range(3):
            part = last.astype(BF16).astype(F32)
            last = last - part
            gate = gate + jnp.where(lane == KV_HEADS + groups * k + row, part, 0.0)
        small_ref[4 + s : 5 + s, :] = jnp.sum(gate, axis=0, keepdims=True)


def fold_kernel(*refs):
    *parts, small_ref, out_ref = refs
    total = sum(ref[...].astype(F32) for ref in parts)
    query = total[:, :1024].astype(BF16)
    extra, key, value = (total[:, 128 * k : 128 * k + 128] for k in (8, 9, 10))
    row = lax.broadcasted_iota(jnp.int32, (8, 128), 0)
    gates = extra[4:8] + small_ref[4:8, :]
    for z in range(out_ref.shape[0]):
        own = jnp.where(row == 5, value[z : z + 1], extra)
        own = jnp.where(row == 4, key[z : z + 1], own)
        own = jnp.where(row == 6, gates[z % 4 : z % 4 + 1], own)
        out_ref[z, :, :1024] = query
        out_ref[z, :, 1024:] = own.astype(BF16)


def attend_kernel(
    sums_ref,
    small_ref,
    gate_ref,
    key_ref,
    value_ref,
    out_ref,
    query_ref,
    scores_ref,
    weights_ref,
):
    tp_rank, z_rank = lax.axis_index("tp"), lax.axis_index("kv_0")
    x_rank = lax.axis_index("kv_1").astype(F32)
    seqs, positions = gate_ref.shape[0], gate_ref.shape[2]
    total = sums_ref[0].astype(F32)
    for piece in range(1, sums_ref.shape[0]):
        total = total + sums_ref[piece].astype(F32)
    extra = total[:, 1024:]
    inverse = lax.rsqrt(extra[:seqs] / D + EPSILON)
    both = jnp.concatenate([inverse, inverse], axis=0)
    for k in range(8):
        tile = total[:, 128 * k : 128 * k + 128] * both
        query_ref[8 * k : 8 * k + 8, :] = tile.astype(BF16).astype(F32)

    def normed(part, gain):
        mean = jnp.sum(part * part, axis=1, keepdims=True) * (1.0 / HEAD)
        return (part * lax.rsqrt(mean + EPSILON) * gain).astype(BF16).astype(F32)

    query_gain, key_gain = small_ref[0:1, :], small_ref[1:2, :]
    lane = lanes_of((8, 128))
    left = lane < HEAD
    early = lax.broadcasted_iota(jnp.int32, (8, 128), 0) < 4
    blocks = positions // 128
    placed = left == early
    parts = {}
    for s in range(seqs):
        for a in range(2):
            heads = query_ref[pl.ds(a * seqs + s, 8, stride=8), :]
            turned = pltpu.roll(heads, HEAD, 1)
            for p, part in enumerate((heads, turned)):
                part = normed(jnp.where(placed, part, 0.0), query_gain)
                parts[s, a, p] = part * HEAD ** (-0.5)
    holds = [
        jnp.broadcast_to(small_ref[3:4, seqs + s : seqs + s + 1], (8, 128)) == x_rank
        for s in range(seqs)
    ]
    own_s, own_a = z_rank % seqs, z_rank // seqs
    scale = sum(jnp.where(own_s == s, inverse[s : s + 1], 0.0) for s in range(seqs))
    key_new = jnp.broadcast_to((extra[4:5] * scale).astype(BF16).astype(F32), (8, 128))
    value_new = (extra[5:6] * scale).astype(BF16).astype(F32)
    key_new = normed(jnp.where(left, key_new, 0.0), key_gain) + normed(
        jnp.where(left, 0.0, key_new), key_gain
    )
    logit = extra[6:7] * scale + small_ref[2:3, :]
    log_gate = jnp.minimum(logit, 0.0) - jnp.log1p(jnp.exp(-jnp.abs(logit)))
    group = jnp.where(early, 2 * own_a, 2 * own_a + 1)
    at = lane - group - KV_HEADS
    groups = KV_HEADS // 2
    last = jnp.logical_or(at == 0, jnp.logical_or(at == groups, at == 2 * groups))
    own = jnp.where(lane == group + groups * tp_rank, log_gate, 0.0) + jnp.where(
        last, extra[6:7], 0.0
    )
    joins = {
        (s, a): jnp.logical_and(holds[s], z_rank == seqs * a + s)
        for s in range(seqs)
        for a in range(2)
    }
    fresh = []
    for p in range(2):
        query = sum(
            jnp.where(z_rank == seqs * a + s, parts[s, a, p], 0.0)
            for s in range(seqs)
            for a in range(2)
        )
        fresh.append(jnp.sum(query * key_new - own, axis=1, keepdims=True))
    zeros = jnp.zeros((16, 128), F32)
    for s in range(seqs):
        query = jnp.concatenate(
            [
                jnp.concatenate([parts[s, 0, 0], parts[s, 0, 1], zeros], axis=0),
                jnp.concatenate([zeros, parts[s, 1, 0], parts[s, 1, 1]], axis=0),
            ],
            axis=1,
        ).astype(BF16)
        scores_ref[32 * s : 32 * s + 32, :] = lax.dot_general(
            query, key_ref[s], (((1,), (0,)), ((), ())), preferred_element_type=F32
        )

    tops = {}
    for s in range(seqs):
        for a in range(2):
            tops[s, a, 0] = tops[s, a, 1] = jnp.full((8, 128), FLOOR / 10, F32)
        for j in range(blocks):
            part = slice(128 * j, 128 * j + 128)
            for a in range(2):
                gate = gate_ref[s, 8 * a : 8 * a + 8, part]
                for p in range(2):
                    at = 32 * s + 16 * a + 8 * p
                    score = scores_ref[at : at + 8, part] - gate
                    scores_ref[at : at + 8, part] = score
                    tops[s, a, p] = jnp.maximum(tops[s, a, p], score)
    rows = [(s, a, p) for s in range(seqs) for a in range(2) for p in range(2)]
    top, weight_new = {}, {}
    for s, a, p in rows:
        most = jnp.max(tops[s, a, p], axis=1, keepdims=True)
        new = jnp.broadcast_to(fresh[p], (8, 128))
        most = jnp.broadcast_to(most, (8, 128))
        top[s, a, p] = jnp.where(joins[s, a], jnp.maximum(most, new), most)
        weight = jnp.where(joins[s, a], jnp.exp(new - top[s, a, p]), 0.0)
        weight_new[s, a, p] = weight.astype(BF16).astype(F32)
    counts, summed = {}, []
    for s in range(seqs):
        for a in range(2):
            counts[s, a, 0] = counts[s, a, 1] = jnp.zeros((8, 128), F32)
            for j in range(blocks):
                part = slice(128 * j, 128 * j + 128)
                both = []
                for p in range(2):
                    at = 32 * s + 16 * a + 8 * p
                    weight = jnp.exp(scores_ref[at : at + 8, part] - top[s, a, p]).astype(BF16)
                    counts[s, a, p] = counts[s, a, p] + weight.astype(F32)
                    both.append(weight)
                at = 32 * s + 16 * a
                weights_ref[at : at + 16, part] = jnp.concatenate(both, axis=0)
        summed.append(
            jnp.dot(
                weights_ref[32 * s : 32 * s + 32, :], value_ref[s], preferred_element_type=F32
            )
        )
    maxima = jnp.zeros((8, 128), F32)
    sums = jnp.zeros((8, 128), F32)
    for s, a, p in rows:
        here = lane == 4 * s + 2 * a + jnp.where(early, p, 1 - p)
        count = jnp.sum(counts[s, a, p], axis=1, keepdims=True) + weight_new[s, a, p]
        maxima = jnp.where(here, top[s, a, p], maxima)
        sums = jnp.where(here, count, sums)
    packed = pack_statistics(maxima, sums)
    for s in range(seqs):
        for a in range(2):
            even, odd = (
                summed[s][16 * a + 8 * p : 16 * a + 8 * p + 8, 128 * a : 128 * a + 128]
                + weight_new[s, a, p] * value_new
                for p in range(2)
            )
            dense = jnp.where(placed, even, pltpu.roll(odd, HEAD, 1)).astype(BF16)
            at = 8 * (2 * s + a)
            out_ref[at : at + 8, :] = dense
    out_ref[64:72, :] = packed


def pack_statistics(maxima, sums):
    first = maxima.astype(BF16).astype(F32)
    second = (maxima - first).astype(BF16).astype(F32)
    third = (maxima - first - second).astype(BF16).astype(F32)
    high = sums.astype(BF16).astype(F32)
    low = (sums - high).astype(BF16).astype(F32)
    packed = first + pltpu.roll(second, 16, 1) + pltpu.roll(third, 32, 1)
    packed = packed + pltpu.roll(high, 48, 1) + pltpu.roll(low, 64, 1)
    return packed.astype(BF16)


def unpack_statistics(packed):
    packed = packed.astype(F32)
    valid = lanes_of((8, 128)) < 16
    maxima = packed + pltpu.roll(packed, 112, 1) + pltpu.roll(packed, 96, 1)
    sums = pltpu.roll(packed, 80, 1) + pltpu.roll(packed, 64, 1)
    return jnp.where(valid, maxima, 0.0), jnp.where(valid, sums, 0.0)


def spread(tile, k):
    left = lanes_of((8, 128)) < HEAD
    return jnp.where(left, tile[:, 2 * k : 2 * k + 1], tile[:, 2 * k + 1 : 2 * k + 2])


def merged(pieces, divide):
    found = [unpack_statistics(piece[64:72, :]) for piece in pieces]
    top = functools.reduce(jnp.maximum, [maxima for maxima, _ in found])
    factors = [jnp.exp(maxima - top) for maxima, _ in found]
    total = sum(factor * sums for factor, (_, sums) in zip(factors, found))
    if divide:
        share = 1.0 / jnp.where(lanes_of((8, 128)) < 16, total, 1.0)
        factors = [factor * share for factor in factors]
    values = []
    for k in range(8):
        values.append(
            sum(
                piece[8 * k : 8 * k + 8, :].astype(F32) * spread(factor, k)
                for piece, factor in zip(pieces, factors)
            )
        )
    return top, total, values


def merge_kernel(*refs):
    out_ref = refs[-1]
    top, total, values = merged(refs[:-1], False)
    packed = pack_statistics(top, total)
    dense = jnp.concatenate(values, axis=0).astype(BF16)
    for copy in range(out_ref.shape[0]):
        out_ref[copy, :64, :] = dense
        out_ref[copy, 64:72, :] = packed


def finish_kernel(in_ref, weight_ref, out_ref, attended_ref):
    values = merged([in_ref.at[i] for i in range(in_ref.shape[0])], True)[2]
    for k in range(8):
        attended_ref[8 * k : 8 * k + 8, :] = values[k]
    attended = jnp.concatenate(
        [attended_ref[pl.ds(k, 4, stride=16), :] for k in range(16)], axis=1
    ).astype(BF16)
    out_ref[...] = jnp.dot(attended, weight_ref[...], preferred_element_type=F32).astype(BF16)


def limit(mebibytes):
    return pltpu.CompilerParams(vmem_limit_bytes=mebibytes << 20)


def in_vmem(count):
    return [pl.BlockSpec(memory_space=VMEM)] * count


def in_hbm(count):
    return [pl.BlockSpec(memory_space=pltpu.HBM)] * count


def held(*arrays):
    return [pltpu.with_memory_space_constraint(array, pltpu.HBM) for array in arrays]


def exchanged(array, axis):
    return lax.all_to_all(array, axis, 0, 0, tiled=True)


def with_peers(array, axis):
    size = lax.axis_size(axis)
    pairs = [[(i, i ^ k) for i in range(size)] for k in range(1, size)]
    return [array] + [lax.ppermute(array, axis, pair) for pair in pairs]


def per_device(
    tokens,
    norm_gain,
    query_weight,
    key_weight,
    value_weight,
    gate_weight,
    gate_bias,
    query_gain,
    key_gain,
    key_cache,
    value_cache,
    gate_cache,
    lengths,
    out_weight,
):
    seqs, columns = tokens.shape
    outer, inner = lax.axis_size("kv_0"), lax.axis_size("kv_1")
    sums = pl.pallas_call(
        project_kernel,
        out_shape=jax.ShapeDtypeStruct((8, 1408), BF16),
        in_specs=in_hbm(6),
        out_specs=in_vmem(1)[0],
        scratch_shapes=[
            VMEM(tokens.shape, BF16),
            VMEM((1, columns), F32),
            VMEM(query_weight.shape, BF16),
            VMEM(key_weight.shape, BF16),
            VMEM(value_weight.shape, BF16),
            VMEM((KV_HEADS, columns), BF16),
            pltpu.SemaphoreType.DMA((5 + PIECES,)),
        ],
        compiler_params=limit(4),
        name="project",
    )(
        *held(
            tokens, norm_gain[None], query_weight, key_weight, value_weight, gate_weight.T
        )
    )
    sums = pl.pallas_call(
        relay_kernel,
        out_shape=jax.ShapeDtypeStruct((8, 1408), BF16),
        in_specs=in_vmem(1),
        out_specs=in_vmem(1)[0],
        compiler_params=limit(4),
        cost_estimate=pl.CostEstimate(
            flops=10**10, bytes_accessed=10**8, transcendentals=0
        ),
        name="relay",
    )(sums)
    small, keys, gates = pl.pallas_call(
        prepare_kernel,
        out_shape=(
            jax.ShapeDtypeStruct((8, 128), F32),
            jax.ShapeDtypeStruct((seqs, key_cache.shape[2], POSITIONS), BF16),
            jax.ShapeDtypeStruct((seqs, 16, POSITIONS), F32),
        ),
        in_specs=in_hbm(5) + in_vmem(1),
        out_specs=tuple(in_vmem(3)),
        scratch_shapes=[
            VMEM((1, KV_HEADS), F32),
            VMEM((1, HEAD), F32),
            VMEM((1, HEAD), F32),
            VMEM((1, seqs), jnp.int32),
            VMEM(gate_cache.shape, F32),
            pltpu.SemaphoreType.DMA((5,)),
        ],
        compiler_params=limit(16),
        cost_estimate=pl.CostEstimate(flops=10**9, bytes_accessed=10**7, transcendentals=0),
        name="prepare",
    )(
        *held(gate_bias[None], query_gain[None], key_gain[None], lengths[None], gate_cache),
        key_cache,
    )
    received, small, keys, gates = lax.optimization_barrier(
        (with_peers(sums, "kv_1"), small, keys, gates)
    )
    sums = pl.pallas_call(
        fold_kernel,
        out_shape=jax.ShapeDtypeStruct((outer, 8, 1152), BF16),
        in_specs=in_vmem(inner + 1),
        out_specs=in_vmem(1)[0],
        compiler_params=limit(4),
        cost_estimate=pl.CostEstimate(
            flops=10**10, bytes_accessed=10**8, transcendentals=0
        ),
        name="fold",
    )(*received, small)
    parts = pl.pallas_call(
        attend_kernel,
        out_shape=jax.ShapeDtypeStruct((72, 128), BF16),
        in_specs=in_vmem(5),
        out_specs=in_vmem(1)[0],
        scratch_shapes=[
            VMEM((64, 128), F32),
            VMEM((32 * seqs, POSITIONS), F32),
            VMEM((32 * seqs, POSITIONS), BF16),
        ],
        compiler_params=limit(24),
        name="attend",
    )(exchanged(sums, "kv_0"), small, gates, keys, value_cache)
    parts = pl.pallas_call(
        merge_kernel,
        out_shape=jax.ShapeDtypeStruct((outer, 72, 128), BF16),
        in_specs=in_vmem(inner),
        out_specs=in_vmem(1)[0],
        compiler_params=limit(4),
        name="merge",
    )(*with_peers(parts, "kv_1"))
    mixed = pl.pallas_call(
        finish_kernel,
        out_shape=jax.ShapeDtypeStruct((seqs, out_weight.shape[1]), BF16),
        in_specs=in_vmem(2),
        out_specs=in_vmem(1)[0],
        scratch_shapes=[VMEM((64, 128), F32)],
        compiler_params=limit(4),
        name="finish",
    )(exchanged(parts, "kv_0"), out_weight)
    other = lax.ppermute(mixed, "tp", [(0, 1), (1, 0)])
    return (mixed.astype(F32) + other.astype(F32)).astype(BF16)


def solution(mesh):
    finer = Mesh(
        mesh.devices.reshape(mesh.shape["dp"], 8, 4, mesh.shape["tp"]), ("dp", "kv_0", "kv_1", "tp")
    )
    in_specs = (
        P("dp", KV),
        P(KV),
        P(KV, "tp"),
        P(KV, "tp"),
        P(KV, "tp"),
        P(),
        P(),
        P(),
        P(),
        P("dp", KV, "tp"),
        P("dp", KV, "tp"),
        P("dp", "tp", KV),
        P("dp"),
        P("tp", KV),
    )
    out_specs = P("dp", KV)
    return jax.shard_map(
        per_device, mesh=finer, in_specs=in_specs, out_specs=out_specs, check_vma=False
    )
```

```python
import functools

import jax
import jax.numpy as jnp
from jax import lax
from jax.experimental import pallas as pl
from jax.experimental.pallas import tpu as pltpu
from jax.sharding import Mesh
from jax.sharding import PartitionSpec as P

D = 4096
HEADS = 64
KV_HEADS = 8
HEAD = 64
POSITIONS = 2048
PIECES = 1
KV = ("kv_0", "kv_1")


EPSILON = 1e-06
FLOOR = -1e30
VMEM = pltpu.VMEM
F32 = jnp.float32
BF16 = jnp.bfloat16


def lanes_of(shape):
    return lax.broadcasted_iota(jnp.int32, shape, 1)


def halves_stacked(part):
    half = part.shape[1] // 2
    return jnp.concatenate([part[:, :half], part[:, half:]], axis=0)


def project_kernel(
    tokens_hbm,
    norm_gain_hbm,
    query_hbm,
    key_hbm,
    value_hbm,
    gate_hbm,
    out_ref,
    tokens_ref,
    norm_gain_ref,
    query_ref,
    key_ref,
    value_ref,
    gate_ref,
    arrived,
):
    seqs, columns = tokens_ref.shape
    kv_rank = lax.axis_index(KV)
    mine = pl.ds(pl.multiple_of(kv_rank * columns, columns), columns)
    pairs = [(tokens_hbm, tokens_ref), (norm_gain_hbm, norm_gain_ref)]
    step = columns // PIECES
    for k in range(PIECES):
        rows = slice(step * k, step * k + step)
        pairs.append((query_hbm.at[rows, :], query_ref.at[rows, :]))
    pairs += [
        (key_hbm, key_ref),
        (value_hbm, value_ref),
        (gate_hbm.at[:, mine], gate_ref),
    ]
    copies = [pltpu.make_async_copy(*pair, arrived.at[k]) for k, pair in enumerate(pairs)]
    for copy in copies:
        copy.start()
    for copy in copies[:2]:
        copy.wait()
    tokens = tokens_ref[...].astype(F32)
    squares = jnp.sum(tokens * tokens, axis=1, keepdims=True)
    scaled = (tokens * norm_gain_ref[...]).astype(BF16)
    for copy in copies[2:]:
        copy.wait()
    query = jnp.dot(scaled, query_ref[...], preferred_element_type=F32)
    key = jnp.dot(scaled, key_ref[...], preferred_element_type=F32)
    value = jnp.dot(scaled, value_ref[...], preferred_element_type=F32)
    rows = gate_ref[...].astype(F32)
    rows = jnp.concatenate([rows, jnp.zeros((128 - KV_HEADS, columns), F32)], axis=0)
    gate = lax.dot_general(
        scaled, rows.astype(BF16), (((1,), (1,)), ((), ())), preferred_element_type=F32
    )
    extra = jnp.concatenate([jnp.broadcast_to(squares, gate.shape), gate], axis=0)
    out_ref[...] = jnp.concatenate(
        [halves_stacked(query), extra, halves_stacked(key), halves_stacked(value)], axis=1
    ).astype(BF16)


def relay_kernel(in_ref, out_ref):
    out_ref[...] = in_ref[...]


def prepare_kernel(
    bias_hbm,
    query_gain_hbm,
    key_gain_hbm,
    lengths_hbm,
    cache_hbm,
    keys_ref,
    small_ref,
    turned_ref,
    gates_ref,
    bias_ref,
    query_gain_ref,
    key_gain_ref,
    lengths_ref,
    cache_ref,
    arrived,
):
    pairs = [
        (bias_hbm, bias_ref),
        (query_gain_hbm, query_gain_ref),
        (key_gain_hbm, key_gain_ref),
        (lengths_hbm, lengths_ref),
        (cache_hbm, cache_ref),
    ]
    copies = [pltpu.make_async_copy(*pair, arrived.at[k]) for k, pair in enumerate(pairs)]
    for copy in copies:
        copy.start()
    for s in range(keys_ref.shape[0]):
        turned_ref[s] = keys_ref[s].T
    for copy in copies:
        copy.wait()
    seqs, groups, positions = cache_ref.shape
    small_ref[0:1, :] = jnp.concatenate([query_gain_ref[...]] * 2, axis=1)
    small_ref[1:2, :] = jnp.concatenate([key_gain_ref[...]] * 2, axis=1)
    small_ref[2:8, :] = jnp.zeros((6, 128), F32)
    small_ref[2:3, 0:KV_HEADS] = bias_ref[...]
    lengths = lengths_ref[...]
    rest = lengths - lax.axis_index(KV) * positions
    small_ref[3:4, 0:seqs] = rest.astype(F32)
    small_ref[3:4, seqs : 2 * seqs] = (
        ((lengths - 1) // positions) % lax.axis_size("kv_1")
    ).astype(F32)
    lane, blocks = lanes_of((8, 128)), positions // 128
    early = lax.broadcasted_iota(jnp.int32, (8, 128), 0) < 4
    for s in range(seqs):
        left = jnp.broadcast_to(rest[0:1, s : s + 1], (8, 128))
        for j in range(blocks):
            part = slice(128 * j, 128 * j + 128)
            live = lane + 128 * j < left
            for a in range(2):
                gate = jnp.where(
                    early,
                    cache_ref[s, 2 * a : 2 * a + 1, part],
                    cache_ref[s, 2 * a + 1 : 2 * a + 2, part],
                )
                gates_ref[s, 8 * a : 8 * a + 8, part] = jnp.where(live, gate, -FLOOR)
    lane = lanes_of((groups, 128))
    row = lax.broadcasted_iota(jnp.int32, (groups, 128), 0)
    place = lanes_of((groups, positions))
    for s in range(seqs):
        last = jnp.where(place == rest[0:1, s : s + 1] - 1, cache_ref[s], 0.0)
        last = jnp.sum(last, axis=1, keepdims=True)
        gate = jnp.zeros((groups, 128), F32)
        for k in range(3):
            part = last.astype(BF16).astype(F32)
            last = last - part
            gate = gate + jnp.where(lane == KV_HEADS + groups * k + row, part, 0.0)
        small_ref[4 + s : 5 + s, :] = jnp.sum(gate, axis=0, keepdims=True)


def fold_kernel(*refs):
    *parts, small_ref, out_ref = refs
    total = sum(ref[...].astype(F32) for ref in parts)
    query = total[:, :1024].astype(BF16)
    extra, key, value = (total[:, 128 * k : 128 * k + 128] for k in (8, 9, 10))
    row = lax.broadcasted_iota(jnp.int32, (8, 128), 0)
    gates = extra[4:8] + small_ref[4:8, :]
    for z in range(out_ref.shape[0]):
        own = jnp.where(row == 5, value[z : z + 1], extra)
        own = jnp.where(row == 4, key[z : z + 1], own)
        own = jnp.where(row == 6, gates[z % 4 : z % 4 + 1], own)
        out_ref[z, :, :1024] = query
        out_ref[z, :, 1024:] = own.astype(BF16)


def attend_kernel(
    sums_ref,
    small_ref,
    gate_ref,
    key_ref,
    value_ref,
    out_ref,
    query_ref,
    scores_ref,
    weights_ref,
):
    tp_rank, z_rank = lax.axis_index("tp"), lax.axis_index("kv_0")
    x_rank = lax.axis_index("kv_1").astype(F32)
    seqs, positions = gate_ref.shape[0], gate_ref.shape[2]
    total = sums_ref[0].astype(F32)
    for piece in range(1, sums_ref.shape[0]):
        total = total + sums_ref[piece].astype(F32)
    extra = total[:, 1024:]
    inverse = lax.rsqrt(extra[:seqs] / D + EPSILON)
    both = jnp.concatenate([inverse, inverse], axis=0)
    for k in range(8):
        tile = total[:, 128 * k : 128 * k + 128] * both
        query_ref[8 * k : 8 * k + 8, :] = tile.astype(BF16).astype(F32)

    def normed(part, gain):
        mean = jnp.sum(part * part, axis=1, keepdims=True) * (1.0 / HEAD)
        return (part * lax.rsqrt(mean + EPSILON) * gain).astype(BF16).astype(F32)

    query_gain, key_gain = small_ref[0:1, :], small_ref[1:2, :]
    lane = lanes_of((8, 128))
    left = lane < HEAD
    early = lax.broadcasted_iota(jnp.int32, (8, 128), 0) < 4
    blocks = positions // 128
    placed = left == early
    parts = {}
    for s in range(seqs):
        for a in range(2):
            heads = query_ref[pl.ds(a * seqs + s, 8, stride=8), :]
            turned = pltpu.roll(heads, HEAD, 1)
            for p, part in enumerate((heads, turned)):
                part = normed(jnp.where(placed, part, 0.0), query_gain)
                parts[s, a, p] = part * HEAD ** (-0.5)
    holds = [
        jnp.broadcast_to(small_ref[3:4, seqs + s : seqs + s + 1], (8, 128)) == x_rank
        for s in range(seqs)
    ]
    own_s, own_a = z_rank % seqs, z_rank // seqs
    scale = sum(jnp.where(own_s == s, inverse[s : s + 1], 0.0) for s in range(seqs))
    key_new = jnp.broadcast_to((extra[4:5] * scale).astype(BF16).astype(F32), (8, 128))
    value_new = (extra[5:6] * scale).astype(BF16).astype(F32)
    key_new = normed(jnp.where(left, key_new, 0.0), key_gain) + normed(
        jnp.where(left, 0.0, key_new), key_gain
    )
    logit = extra[6:7] * scale + small_ref[2:3, :]
    log_gate = jnp.minimum(logit, 0.0) - jnp.log1p(jnp.exp(-jnp.abs(logit)))
    group = jnp.where(early, 2 * own_a, 2 * own_a + 1)
    at = lane - group - KV_HEADS
    groups = KV_HEADS // 2
    last = jnp.logical_or(at == 0, jnp.logical_or(at == groups, at == 2 * groups))
    own = jnp.where(lane == group + groups * tp_rank, log_gate, 0.0) + jnp.where(
        last, extra[6:7], 0.0
    )
    joins = {
        (s, a): jnp.logical_and(holds[s], z_rank == seqs * a + s)
        for s in range(seqs)
        for a in range(2)
    }
    fresh = []
    for p in range(2):
        query = sum(
            jnp.where(z_rank == seqs * a + s, parts[s, a, p], 0.0)
            for s in range(seqs)
            for a in range(2)
        )
        fresh.append(jnp.sum(query * key_new - own, axis=1, keepdims=True))
    zeros = jnp.zeros((16, 128), F32)
    for s in range(seqs):
        query = jnp.concatenate(
            [
                jnp.concatenate([parts[s, 0, 0], parts[s, 0, 1], zeros], axis=0),
                jnp.concatenate([zeros, parts[s, 1, 0], parts[s, 1, 1]], axis=0),
            ],
            axis=1,
        ).astype(BF16)
        scores_ref[32 * s : 32 * s + 32, :] = lax.dot_general(
            query, key_ref[s], (((1,), (0,)), ((), ())), preferred_element_type=F32
        )

    tops = {}
    for s in range(seqs):
        for a in range(2):
            tops[s, a, 0] = tops[s, a, 1] = jnp.full((8, 128), FLOOR / 10, F32)
        for j in range(blocks):
            part = slice(128 * j, 128 * j + 128)
            for a in range(2):
                gate = gate_ref[s, 8 * a : 8 * a + 8, part]
                for p in range(2):
                    at = 32 * s + 16 * a + 8 * p
                    score = scores_ref[at : at + 8, part] - gate
                    scores_ref[at : at + 8, part] = score
                    tops[s, a, p] = jnp.maximum(tops[s, a, p], score)
    rows = [(s, a, p) for s in range(seqs) for a in range(2) for p in range(2)]
    top, weight_new = {}, {}
    for s, a, p in rows:
        most = jnp.max(tops[s, a, p], axis=1, keepdims=True)
        new = jnp.broadcast_to(fresh[p], (8, 128))
        most = jnp.broadcast_to(most, (8, 128))
        top[s, a, p] = jnp.where(joins[s, a], jnp.maximum(most, new), most)
        weight = jnp.where(joins[s, a], jnp.exp(new - top[s, a, p]), 0.0)
        weight_new[s, a, p] = weight.astype(BF16).astype(F32)
    counts, summed = {}, []
    for s in range(seqs):
        for a in range(2):
            counts[s, a, 0] = counts[s, a, 1] = jnp.zeros((8, 128), F32)
            for j in range(blocks):
                part = slice(128 * j, 128 * j + 128)
                both = []
                for p in range(2):
                    at = 32 * s + 16 * a + 8 * p
                    weight = jnp.exp(scores_ref[at : at + 8, part] - top[s, a, p]).astype(BF16)
                    counts[s, a, p] = counts[s, a, p] + weight.astype(F32)
                    both.append(weight)
                at = 32 * s + 16 * a
                weights_ref[at : at + 16, part] = jnp.concatenate(both, axis=0)
        summed.append(
            jnp.dot(
                weights_ref[32 * s : 32 * s + 32, :], value_ref[s], preferred_element_type=F32
            )
        )
    maxima = jnp.zeros((8, 128), F32)
    sums = jnp.zeros((8, 128), F32)
    for s, a, p in rows:
        here = lane == 4 * s + 2 * a + jnp.where(early, p, 1 - p)
        count = jnp.sum(counts[s, a, p], axis=1, keepdims=True) + weight_new[s, a, p]
        maxima = jnp.where(here, top[s, a, p], maxima)
        sums = jnp.where(here, count, sums)
    packed = pack_statistics(maxima, sums)
    for s in range(seqs):
        for a in range(2):
            even, odd = (
                summed[s][16 * a + 8 * p : 16 * a + 8 * p + 8, 128 * a : 128 * a + 128]
                + weight_new[s, a, p] * value_new
                for p in range(2)
            )
            dense = jnp.where(placed, even, pltpu.roll(odd, HEAD, 1)).astype(BF16)
            at = 8 * (2 * s + a)
            for copy in range(out_ref.shape[0]):
                out_ref[copy, at : at + 8, :] = dense
    for copy in range(out_ref.shape[0]):
        out_ref[copy, 64:72, :] = packed


def pack_statistics(maxima, sums):
    first = maxima.astype(BF16).astype(F32)
    second = (maxima - first).astype(BF16).astype(F32)
    third = (maxima - first - second).astype(BF16).astype(F32)
    high = sums.astype(BF16).astype(F32)
    low = (sums - high).astype(BF16).astype(F32)
    packed = first + pltpu.roll(second, 16, 1) + pltpu.roll(third, 32, 1)
    packed = packed + pltpu.roll(high, 48, 1) + pltpu.roll(low, 64, 1)
    return packed.astype(BF16)


def unpack_statistics(packed):
    packed = packed.astype(F32)
    valid = lanes_of((8, 128)) < 16
    maxima = packed + pltpu.roll(packed, 112, 1) + pltpu.roll(packed, 96, 1)
    sums = pltpu.roll(packed, 80, 1) + pltpu.roll(packed, 64, 1)
    return jnp.where(valid, maxima, 0.0), jnp.where(valid, sums, 0.0)


def spread(tile, k):
    left = lanes_of((8, 128)) < HEAD
    return jnp.where(left, tile[:, 2 * k : 2 * k + 1], tile[:, 2 * k + 1 : 2 * k + 2])


def merged(pieces, divide):
    found = [unpack_statistics(piece[64:72, :]) for piece in pieces]
    top = functools.reduce(jnp.maximum, [maxima for maxima, _ in found])
    factors = [jnp.exp(maxima - top) for maxima, _ in found]
    total = sum(factor * sums for factor, (_, sums) in zip(factors, found))
    if divide:
        share = 1.0 / jnp.where(lanes_of((8, 128)) < 16, total, 1.0)
        factors = [factor * share for factor in factors]
    values = []
    for k in range(8):
        values.append(
            sum(
                piece[8 * k : 8 * k + 8, :].astype(F32) * spread(factor, k)
                for piece, factor in zip(pieces, factors)
            )
        )
    return top, total, values


def merge_kernel(in_ref, out_ref):
    top, total, values = merged([in_ref.at[i] for i in range(in_ref.shape[0])], False)
    out_ref[:64, :] = jnp.concatenate(values, axis=0).astype(BF16)
    out_ref[64:72, :] = pack_statistics(top, total)


def finish_kernel(*refs):
    *pieces, weight_ref, out_ref, attended_ref = refs
    values = merged(pieces, True)[2]
    for k in range(8):
        attended_ref[8 * k : 8 * k + 8, :] = values[k]
    attended = jnp.concatenate(
        [attended_ref[pl.ds(k, 4, stride=16), :] for k in range(16)], axis=1
    ).astype(BF16)
    out_ref[...] = jnp.dot(attended, weight_ref[...], preferred_element_type=F32).astype(BF16)


def limit(mebibytes):
    return pltpu.CompilerParams(vmem_limit_bytes=mebibytes << 20)


def in_vmem(count):
    return [pl.BlockSpec(memory_space=VMEM)] * count


def in_hbm(count):
    return [pl.BlockSpec(memory_space=pltpu.HBM)] * count


def held(*arrays):
    return [pltpu.with_memory_space_constraint(array, pltpu.HBM) for array in arrays]


def exchanged(array, axis):
    return lax.all_to_all(array, axis, 0, 0, tiled=True)


def with_peers(array, axis):
    size = lax.axis_size(axis)
    pairs = [[(i, i ^ k) for i in range(size)] for k in range(1, size)]
    return [array] + [lax.ppermute(array, axis, pair) for pair in pairs]


def per_device(
    tokens,
    norm_gain,
    query_weight,
    key_weight,
    value_weight,
    gate_weight,
    gate_bias,
    query_gain,
    key_gain,
    key_cache,
    value_cache,
    gate_cache,
    lengths,
    out_weight,
):
    seqs, columns = tokens.shape
    outer, inner = lax.axis_size("kv_0"), lax.axis_size("kv_1")
    sums = pl.pallas_call(
        project_kernel,
        out_shape=jax.ShapeDtypeStruct((8, 1408), BF16),
        in_specs=in_hbm(6),
        out_specs=in_vmem(1)[0],
        scratch_shapes=[
            VMEM(tokens.shape, BF16),
            VMEM((1, columns), F32),
            VMEM(query_weight.shape, BF16),
            VMEM(key_weight.shape, BF16),
            VMEM(value_weight.shape, BF16),
            VMEM((KV_HEADS, columns), BF16),
            pltpu.SemaphoreType.DMA((5 + PIECES,)),
        ],
        compiler_params=limit(4),
        name="project",
    )(
        *held(
            tokens, norm_gain[None], query_weight, key_weight, value_weight, gate_weight.T
        )
    )
    sums = pl.pallas_call(
        relay_kernel,
        out_shape=jax.ShapeDtypeStruct((8, 1408), BF16),
        in_specs=in_vmem(1),
        out_specs=in_vmem(1)[0],
        compiler_params=limit(4),
        cost_estimate=pl.CostEstimate(
            flops=10**10, bytes_accessed=10**8, transcendentals=0
        ),
        name="relay",
    )(sums)
    small, keys, gates = pl.pallas_call(
        prepare_kernel,
        out_shape=(
            jax.ShapeDtypeStruct((8, 128), F32),
            jax.ShapeDtypeStruct((seqs, key_cache.shape[2], POSITIONS), BF16),
            jax.ShapeDtypeStruct((seqs, 16, POSITIONS), F32),
        ),
        in_specs=in_hbm(5) + in_vmem(1),
        out_specs=tuple(in_vmem(3)),
        scratch_shapes=[
            VMEM((1, KV_HEADS), F32),
            VMEM((1, HEAD), F32),
            VMEM((1, HEAD), F32),
            VMEM((1, seqs), jnp.int32),
            VMEM(gate_cache.shape, F32),
            pltpu.SemaphoreType.DMA((5,)),
        ],
        compiler_params=limit(16),
        cost_estimate=pl.CostEstimate(flops=10**9, bytes_accessed=10**7, transcendentals=0),
        name="prepare",
    )(
        *held(gate_bias[None], query_gain[None], key_gain[None], lengths[None], gate_cache),
        key_cache,
    )
    received, small, keys, gates = lax.optimization_barrier(
        (with_peers(sums, "kv_1"), small, keys, gates)
    )
    sums = pl.pallas_call(
        fold_kernel,
        out_shape=jax.ShapeDtypeStruct((outer, 8, 1152), BF16),
        in_specs=in_vmem(inner + 1),
        out_specs=in_vmem(1)[0],
        compiler_params=limit(4),
        cost_estimate=pl.CostEstimate(
            flops=10**10, bytes_accessed=10**8, transcendentals=0
        ),
        name="fold",
    )(*received, small)
    parts = pl.pallas_call(
        attend_kernel,
        out_shape=jax.ShapeDtypeStruct((outer, 72, 128), BF16),
        in_specs=in_vmem(5),
        out_specs=in_vmem(1)[0],
        scratch_shapes=[
            VMEM((64, 128), F32),
            VMEM((32 * seqs, POSITIONS), F32),
            VMEM((32 * seqs, POSITIONS), BF16),
        ],
        compiler_params=limit(24),
        name="attend",
    )(exchanged(sums, "kv_0"), small, gates, keys, value_cache)
    parts = pl.pallas_call(
        merge_kernel,
        out_shape=jax.ShapeDtypeStruct((72, 128), BF16),
        in_specs=in_vmem(1),
        out_specs=in_vmem(1)[0],
        compiler_params=limit(4),
        name="merge",
    )(exchanged(parts, "kv_0"))
    mixed = pl.pallas_call(
        finish_kernel,
        out_shape=jax.ShapeDtypeStruct((seqs, out_weight.shape[1]), BF16),
        in_specs=in_vmem(inner + 1),
        out_specs=in_vmem(1)[0],
        scratch_shapes=[VMEM((64, 128), F32)],
        compiler_params=limit(4),
        name="finish",
    )(*with_peers(parts, "kv_1"), out_weight)
    other = lax.ppermute(mixed, "tp", [(0, 1), (1, 0)])
    return (mixed.astype(F32) + other.astype(F32)).astype(BF16)


def solution(mesh):
    finer = Mesh(
        mesh.devices.reshape(mesh.shape["dp"], 8, 4, mesh.shape["tp"]), ("dp", "kv_0", "kv_1", "tp")
    )
    in_specs = (
        P("dp", KV),
        P(KV),
        P(KV, "tp"),
        P(KV, "tp"),
        P(KV, "tp"),
        P(),
        P(),
        P(),
        P(),
        P("dp", KV, "tp"),
        P("dp", KV, "tp"),
        P("dp", "tp", KV),
        P("dp"),
        P("tp", KV),
    )
    out_specs = P("dp", KV)
    return jax.shard_map(
        per_device, mesh=finer, in_specs=in_specs, out_specs=out_specs, check_vma=False
    )
```
